128 devices in a mesh: sp: 16 (over z, y), tp: 8 (over x, core).
Axes of the slice: x: 4, y: 4, z: 4, core: 2. Of those that a mesh axis runs over, the one named last changes fastest.
Arguments:
- hidden_activations: bfloat16 [12288, 4096], P(('sp', 'tp')), may hold values from -6 to 6
- entry_rescale_vector: bfloat16 [4096], replicated, may hold values from 0.099609375 to 1.8984375
- probe_matrix: bfloat16 [4096, 2048], P('sp', 'tp'), may hold values from -0.09375 to 0.09375
- lookup_address_matrix: bfloat16 [4096, 2048], P('sp', 'tp'), may hold values from -0.09375 to 0.09375
- payload_matrix: bfloat16 [4096, 4096], P('sp', 'tp'), may hold values from -0.09375 to 0.09375
- postfilter_switch_matrix: bfloat16 [4096, 4096], P('sp', 'tp'), may hold values from -0.09375 to 0.09375
- prefilter_switch_matrix: bfloat16 [4096, 4096], P('sp', 'tp'), may hold values from -0.09375 to 0.09375
- filter_source_matrix: bfloat16 [4096, 4096], P('sp', 'tp'), may hold values from -0.09375 to 0.09375
- forget_left_factor: bfloat16 [4096, 64], replicated, may hold values from -0.09375 to 0.09375
- forget_right_factor: bfloat16 [64, 2048], P(None, 'tp'), may hold values from -0.75 to 0.75
- forget_offset_per_feature: float32 [2048], P('tp'), may hold values from -1 to 12
- forget_spike_additions: float32 [16, 12288], P('tp', 'sp'), may hold values from -3 to 0
- subspace_rescale_vector: bfloat16 [16, 256], P('tp'), may hold values from 0.099609375 to 1.8984375
- depthwise_filter_taps: bfloat16 [3, 4096], P(None, 'tp'), may hold values from -3.5 to 3.5
- mixer_result_matrix: bfloat16 [4096, 4096], P('tp'), may hold values from -0.09375 to 0.09375
- filter_result_matrix: bfloat16 [4096, 4096], P('tp'), may hold values from -0.09375 to 0.09375
Outputs:
- mixed: bfloat16 [12288, 4096], P(('sp', 'tp'))
The draws below stay inside these ranges and needn't reach their ends.
All inputs are finite; a program needn't handle non-finite values.
Results may differ from the reference program's by a relative error of at most 0.02.
Values may be sent and summed in bfloat16 or wider, within the bound.
A program may use at most 128 MiB of HBM per device.

```python
import jax
import jax.numpy as jnp
from jax import lax

MODEL = 4096
HEAD_TOTAL = 16
KEY_CHANNELS = 128
VALUE_DIM = 256
CONV_DIM = 4096
DECAY_RANK = 64
TAPS = 3
BLOCK = 64
TOKENS_DEV = 768
TOKEN_LENGTH = 12288
KEY_WIDTH = 2048
VALUE_WIDTH = 4096
N_TP = 8


def draw_forget_offset_per_feature(key, part):
    key_slow = jax.random.fold_in(key, 11)
    key_fast = jax.random.fold_in(key, 12)
    key_pick = jax.random.fold_in(key, 13)
    slow_heads = jax.random.randint(key_pick, (HEAD_TOTAL,), 0, 10) < 5
    slow_values = jnp.log(TOKEN_LENGTH / 8.0) + jax.random.uniform(key_slow, (HEAD_TOTAL, KEY_CHANNELS), jnp.float32, -0.5, 0.5)
    fast_values = jax.random.uniform(key_fast, (HEAD_TOTAL, KEY_CHANNELS), jnp.float32, -0.5, 1.5)
    chosen = jnp.where(slow_heads[:, None], slow_values, fast_values)
    return chosen.reshape(HEAD_TOTAL * KEY_CHANNELS).astype(jnp.float32)


def draw_forget_spike_additions(key, part):
    key_rate = jax.random.fold_in(key, 21)
    key_where = jax.random.fold_in(key, 22)
    key_size = jax.random.fold_in(key, 23)
    block_total = TOKEN_LENGTH // TOKENS_DEV
    rates = jnp.exp(jax.random.uniform(key_rate, (HEAD_TOTAL, block_total), jnp.float32, jnp.log(0.05), jnp.log(0.4)))
    starting_figure = -jnp.repeat(rates / TOKEN_LENGTH, TOKENS_DEV, axis=1)
    where = jax.random.randint(key_where, (HEAD_TOTAL, 3), 0, TOKEN_LENGTH)
    extent_sequence = jnp.log(jax.random.uniform(key_size, (HEAD_TOTAL, 3), jnp.float32, 0.5, 0.8))
    positions = jnp.arange(TOKEN_LENGTH, dtype=jnp.int32)
    agreeing_tally = (positions[None, None, :] == where[:, :, None]).astype(jnp.float32)
    spike_amounts = jnp.sum(agreeing_tally * extent_sequence[:, :, None], axis=1)
    return (starting_figure + spike_amounts).astype(jnp.float32)


def levels(stream_key, extent, pieces, low, largest):
    factor_of = 1.0
    for position, parts in pieces:
        steps = jax.random.uniform(jax.random.fold_in(jax.random.fold_in(stream_key, 6), position), (parts,), jnp.float32, low / len(pieces), largest / len(pieces))
        factor_of = factor_of * jnp.repeat(jnp.exp(steps), extent[position] // parts).reshape((-1,) + (1,) * (len(extent) - 1 - position))
    return factor_of


def scatter_about(key, shape, spread, bound, pieces=(), kind=jnp.bfloat16):
    level = levels(key, shape, pieces, -0.22, 0.18) if pieces else 1.0
    drawn = jax.random.normal(key, shape, jnp.float32) * spread * level
    return jnp.minimum(jnp.maximum(drawn, -bound), bound).astype(kind)


def setup_inputs(seed: int = 0) -> dict:
    key_of = jax.random.split(jax.random.key(seed), 17)
    return {
        "hidden_activations": scatter_about(key_of[0], (TOKEN_LENGTH, MODEL), 1.0, 6.0, ((0, 128),)),
        "entry_rescale_vector": jnp.clip(1.0 + 0.18 * jax.random.normal(key_of[1], (MODEL,), jnp.float32), 0.099609375, 1.8984375).astype(jnp.bfloat16),
        "probe_matrix": scatter_about(key_of[2], (MODEL, KEY_WIDTH), MODEL ** -0.5, 0.09375, ((0, 16), (1, 8))),
        "lookup_address_matrix": scatter_about(key_of[3], (MODEL, KEY_WIDTH), MODEL ** -0.5, 0.09375, ((0, 16), (1, 8))),
        "payload_matrix": scatter_about(key_of[4], (MODEL, VALUE_WIDTH), MODEL ** -0.5, 0.09375, ((0, 16), (1, 8))),
        "postfilter_switch_matrix": scatter_about(key_of[5], (MODEL, CONV_DIM), MODEL ** -0.5, 0.09375, ((0, 16), (1, 8))),
        "prefilter_switch_matrix": scatter_about(key_of[6], (MODEL, CONV_DIM), MODEL ** -0.5, 0.09375, ((0, 16), (1, 8))),
        "filter_source_matrix": scatter_about(key_of[7], (MODEL, CONV_DIM), MODEL ** -0.5, 0.09375, ((0, 16), (1, 8))),
        "forget_left_factor": scatter_about(key_of[8], (MODEL, DECAY_RANK), MODEL ** -0.5, 0.09375),
        "forget_right_factor": scatter_about(key_of[9], (DECAY_RANK, KEY_WIDTH), DECAY_RANK ** -0.5, 0.75, ((1, 8),)),
        "forget_offset_per_feature": draw_forget_offset_per_feature(jax.random.fold_in(key_of[16], 71), 0),
        "forget_spike_additions": draw_forget_spike_additions(jax.random.fold_in(key_of[16], 71), 0),
        "subspace_rescale_vector": jnp.clip(1.0 + 0.18 * jax.random.normal(key_of[12], (HEAD_TOTAL, VALUE_DIM), jnp.float32), 0.099609375, 1.8984375).astype(jnp.bfloat16),
        "depthwise_filter_taps": scatter_about(key_of[13], (TAPS, CONV_DIM), TAPS ** -0.5, 3.5, ((1, 8),)),
        "mixer_result_matrix": scatter_about(key_of[14], (VALUE_WIDTH, MODEL), VALUE_WIDTH ** -0.5, 0.09375, ((0, 8),)),
        "filter_result_matrix": scatter_about(key_of[15], (CONV_DIM, MODEL), CONV_DIM ** -0.5, 0.09375, ((0, 8),)),
    }


epsilon = 1e-06
softness_scale = 16.0

def row_norm(rows, gain):
    rows_f = rows.astype(jnp.float32)
    meansq = lax.optimization_barrier(jnp.mean(rows_f * rows_f, axis=-1, keepdims=True))
    return rows_f * lax.rsqrt(meansq + epsilon) * gain.astype(jnp.float32)

def block_terms(query_rows, key_rows, value_rows, forget_log_rate):
    length_value, head_number, key_dim = query_rows.shape
    value_dim = value_rows.shape[2]
    block_count = length_value // BLOCK
    key_shape = (block_count, BLOCK, head_number, key_dim)
    query_f32 = query_rows.astype(jnp.float32).reshape(key_shape) * key_dim ** (-0.5)
    key_f32 = key_rows.astype(jnp.float32).reshape(key_shape)
    value_f32 = value_rows.astype(jnp.float32).reshape(block_count, BLOCK, head_number, value_dim)
    within = jnp.cumsum(forget_log_rate.reshape(key_shape), axis=1)
    block_end = within[:, -1]
    query_decayed = query_f32 * jnp.exp(within)
    key_inverse = key_f32 * jnp.exp(-within)
    key_tail = key_f32 * jnp.exp(block_end[:, None] - within)
    highest = lax.Precision.HIGHEST
    scores = jnp.einsum('nihd,njhd->nhij', query_decayed, key_inverse, precision=highest)
    causal = jnp.tril(jnp.ones((BLOCK, BLOCK), dtype=bool))
    scores = jnp.where(causal, scores, 0.0)
    inside = jnp.einsum('nhij,njhv->nihv', scores, value_f32, precision=highest)
    updates = jnp.einsum('njhd,njhv->nhdv', key_tail, value_f32, precision=highest)

    def advance(state, pair):
        decay_now, update_now = pair
        return (jnp.exp(decay_now)[..., None] * state + update_now, state)
    start_state = jnp.zeros((head_number, key_dim, value_dim), jnp.float32)
    final_state, state_in = lax.scan(advance, start_state, (block_end, updates))
    carried = jnp.einsum('nihd,nhdv->nihv', query_decayed, state_in, precision=highest)
    return (inside + carried, query_decayed, block_end, final_state)

def reference(hidden_activations, entry_rescale_vector, probe_matrix, lookup_address_matrix, payload_matrix, postfilter_switch_matrix, prefilter_switch_matrix, filter_source_matrix, forget_left_factor, forget_right_factor, forget_offset_per_feature, forget_spike_additions, subspace_rescale_vector, depthwise_filter_taps, mixer_result_matrix, filter_result_matrix):
    normalized_input = row_norm(hidden_activations, entry_rescale_vector).astype(jnp.bfloat16)

    def project(weight):
        return jnp.dot(normalized_input, weight, preferred_element_type=jnp.float32).astype(jnp.bfloat16)
    queries = project(probe_matrix)
    key_rows = project(lookup_address_matrix)
    value_rows = project(payload_matrix)
    outer = project(postfilter_switch_matrix)
    inner = project(prefilter_switch_matrix)
    conv_in = project(filter_source_matrix)
    low_rank = project(forget_left_factor)
    gate_preactivation = jnp.dot(low_rank, forget_right_factor, preferred_element_type=jnp.float32) + forget_offset_per_feature
    forget_log_rate = (jax.nn.log_sigmoid(gate_preactivation) / softness_scale).reshape(TOKEN_LENGTH, HEAD_TOTAL, KEY_CHANNELS)
    forget_log_rate = forget_log_rate + jnp.transpose(forget_spike_additions)[:, :, None]
    attended, unused_q, unused_e, unused_s = block_terms(queries.reshape(TOKEN_LENGTH, HEAD_TOTAL, KEY_CHANNELS), key_rows.reshape(TOKEN_LENGTH, HEAD_TOTAL, KEY_CHANNELS), value_rows.reshape(TOKEN_LENGTH, HEAD_TOTAL, VALUE_DIM), forget_log_rate)
    attended = attended.reshape(TOKEN_LENGTH, HEAD_TOTAL, VALUE_DIM)
    mixed_attn = row_norm(attended, subspace_rescale_vector).astype(jnp.bfloat16).reshape(TOKEN_LENGTH, HEAD_TOTAL * VALUE_DIM)
    gated_in = (inner.astype(jnp.float32) * conv_in.astype(jnp.float32)).astype(jnp.bfloat16)
    padded = jnp.concatenate([jnp.zeros((TAPS - 1, CONV_DIM), jnp.bfloat16), gated_in], axis=0)
    taps_f32 = depthwise_filter_taps.astype(jnp.float32)
    conv_sum = jnp.zeros((TOKEN_LENGTH, CONV_DIM), jnp.float32)
    for tap_index in range(TAPS):
        conv_sum = conv_sum + taps_f32[tap_index] * padded[tap_index:tap_index + TOKEN_LENGTH].astype(jnp.float32)
    mixed_conv = (conv_sum * outer.astype(jnp.float32)).astype(jnp.bfloat16)
    head_cols = HEAD_TOTAL * VALUE_DIM // N_TP
    conv_cols = CONV_DIM // N_TP
    running = jnp.zeros((TOKEN_LENGTH, MODEL), jnp.float32)
    for group in range(N_TP):
        term = jnp.dot(mixed_attn[:, group * head_cols:(group + 1) * head_cols], mixer_result_matrix[group * head_cols:(group + 1) * head_cols], preferred_element_type=jnp.float32)
        term = term + jnp.dot(mixed_conv[:, group * conv_cols:(group + 1) * conv_cols], filter_result_matrix[group * conv_cols:(group + 1) * conv_cols], preferred_element_type=jnp.float32)
        rounded = lax.optimization_barrier(term.astype(jnp.bfloat16))
        running = running + rounded.astype(jnp.float32)
    return running.astype(jnp.bfloat16)
```

```python
import functools

import jax
import jax.numpy as jnp
from jax import lax
from jax.experimental import pallas as pl
from jax.experimental.pallas import tpu as pltpu
from jax.sharding import Mesh
from jax.sharding import PartitionSpec as P

MESH = pl.DeviceIdType.MESH
SP = ("sp_0", "sp_1")
SP_TP = ("sp_0", "sp_1", "tp")
F32 = jnp.float32
BF16 = jnp.bfloat16
HIGHEST = lax.Precision.HIGHEST

BLOCK = 64
ROWS = 96
TOK = 768
MODEL = 4096
KB = 256
QA, CA = 512, 768
KEY, VAL = 128, 256
EPS = 1e-06
DELTA = (0, 3, 1, 2)


def nt(a, b):
    return lax.dot_general(a, b, (((1,), (1,)), ((), ())), preferred_element_type=F32)


def tn(a, b):
    return lax.dot_general(a, b, (((0,), (0,)), ((), ())), preferred_element_type=F32)


def mm(a, b):
    return jnp.dot(a, b, preferred_element_type=F32)


def front_kernel(
    x_in,
    gain,
    w_q,
    w_k,
    w_v,
    w_out,
    w_in,
    w_src,
    left,
    right,
    offset,
    spikes,
    head_gain,
    taps,
    attn_out,
    conv_out,
    xs,
    qa,
    qb,
    ca,
    cb,
    acc_a,
    acc_b,
    qrows,
    krows,
    vrows,
    rate,
    inside,
    q_far,
    state,
    prefix,
    st_send,
    dec_send,
    st_recv,
    dec_recv,
    gated,
    load_sem,
    w_send,
    w_recv,
    x_send,
    x_recv,
    s_send,
    s_recv,
    h_sem,
):
    z = lax.axis_index("sp_0")
    y = lax.axis_index("sp_1")
    t = lax.axis_index("tp")
    core = t % 2
    xi = t // 2
    sib = xi * 2 + (1 - core)

    def at_z(d):
        return {"sp_0": (z + d) % 4}

    def at_y(d):
        return {"sp_1": (y + d) % 4}

    def at_x(d):
        return {"tp": ((xi + d) % 4) * 2 + core}

    sp = z * 4 + y
    sp_next = (sp + 1) % 16
    sp_prev = (sp + 15) % 16
    to_next = {"sp_0": sp_next // 4, "sp_1": sp_next % 4}
    to_prev = {"sp_0": sp_prev // 4, "sp_1": sp_prev % 4}
    to_sib = {"tp": sib}

    own = pl.ds(pl.multiple_of(sp * KB, KB), KB)
    own_rows = pl.multiple_of(t * ROWS, 32)
    loads = [
        pltpu.make_async_copy(x_in, xs.at[pl.ds(own_rows, ROWS), :], load_sem.at[0]),
        pltpu.make_async_copy(w_q, qa.at[own, 0:256], load_sem.at[1]),
        pltpu.make_async_copy(w_k, qa.at[own, 256:512], load_sem.at[2]),
        pltpu.make_async_copy(w_v, qb.at[own, :], load_sem.at[3]),
        pltpu.make_async_copy(w_out, ca.at[own, 0:512], load_sem.at[4]),
        pltpu.make_async_copy(w_in.at[:, 0:256], ca.at[own, 512:768], load_sem.at[5]),
        pltpu.make_async_copy(w_in.at[:, 256:512], cb.at[own, 0:256], load_sem.at[6]),
        pltpu.make_async_copy(w_src, cb.at[own, 256:768], load_sem.at[7]),
    ]
    for c in loads:
        c.start()

    barrier = pltpu.get_barrier_semaphore()
    peers = [at_z(1), at_z(2), at_z(3), at_y(1), at_y(2), at_y(3), at_x(1), at_x(3), to_sib, to_next, to_prev]
    for p in peers:
        pl.semaphore_signal(barrier, inc=1, device_id=p, device_id_type=MESH)

    loads[0].wait()

    def norm_rows(i, _):
        r = pl.ds(pl.multiple_of(own_rows + i * 16, 16), 16)
        v = xs[r, :].astype(F32)
        ms = jnp.mean(v * v, axis=-1, keepdims=True)
        xs[r, :] = (v * lax.rsqrt(ms + EPS) * gain[...]).astype(BF16)
        return 0

    lax.fori_loop(0, ROWS // 16, norm_rows, 0)
    for c in loads[1:]:
        c.wait()
    pl.semaphore_wait(barrier, len(peers))

    def x_copy(slot, sender_x, row, rows, dst, sender_core=None):
        g = sender_x * 2 + (core if sender_core is None else sender_core)
        ref = xs.at[pl.ds(pl.multiple_of(g * ROWS + row, 16), rows), :]
        return pltpu.make_async_remote_copy(
            src_ref=ref,
            dst_ref=ref,
            send_sem=x_send.at[slot],
            recv_sem=x_recv.at[slot],
            device_id=dst,
            device_id_type=MESH,
        )

    started = []

    def go(c):
        c.start()
        started.append(c)

    right_x, left_x = at_x(1), at_x(3)
    xm, xp, xf = (xi + 3) % 4, (xi + 1) % 4, (xi + 2) % 4

    bufs = {("q", 0): qa, ("q", 1): qb, ("c", 0): ca, ("c", 1): cb}

    def blk(path, du, dv, row=0, rows=KB):
        if path == 0:
            j = ((z + du) % 4) * 4 + (y + dv) % 4
        else:
            j = ((z + dv) % 4) * 4 + (y + du) % 4
        return pl.ds(pl.multiple_of(j * KB + row, 128), rows)

    def w_copy(group, path, slot, du, dv, axis, step, row=0, rows=KB):
        ref = bufs[group, path].at[blk(path, du, dv, row, rows), :]
        along_z = (axis == 0) == (path == 0)
        s = (0 if group == "q" else 2) + path
        return pltpu.make_async_remote_copy(
            src_ref=ref,
            dst_ref=ref,
            send_sem=w_send.at[s, slot],
            recv_sem=w_recv.at[s, slot],
            device_id=at_z(step) if along_z else at_y(step),
            device_id_type=MESH,
        )

    def send_first(g):
        for p in (0, 1):
            go(w_copy(g, p, 0, 0, 0, 0, 1))
            go(w_copy(g, p, 1, 0, 0, 0, 3))

    def wait_first(g):
        for p in (0, 1):
            w_copy(g, p, 0, 3, 0, 0, 1).wait_recv()
            go(w_copy(g, p, 2, 3, 0, 0, 1, 0, 128))
            w_copy(g, p, 1, 1, 0, 0, 3).wait_recv()
            go(w_copy(g, p, 3, 1, 0, 0, 3, 128, 128))

    def wait_first_halves(g):
        for p in (0, 1):
            w_copy(g, p, 2, 2, 0, 0, 1, 0, 128).wait_recv()
            w_copy(g, p, 3, 2, 0, 0, 3, 128, 128).wait_recv()

    def send_second(g, k):
        for p in (0, 1):
            go(w_copy(g, p, 4 + 2 * k, DELTA[k], 0, 1, 1))
            go(w_copy(g, p, 5 + 2 * k, DELTA[k], 0, 1, 3))

    def wait_second(g, k):
        for p in (0, 1):
            w_copy(g, p, 4 + 2 * k, DELTA[k], 3, 1, 1).wait_recv()
            go(w_copy(g, p, 12 + 2 * k, DELTA[k], 3, 1, 1, 0, 128))
            w_copy(g, p, 5 + 2 * k, DELTA[k], 1, 1, 3).wait_recv()
            go(w_copy(g, p, 13 + 2 * k, DELTA[k], 1, 1, 3, 128, 128))

    def wait_second_halves(g, k):
        for p in (0, 1):
            w_copy(g, p, 12 + 2 * k, DELTA[k], 2, 1, 1, 0, 128).wait_recv()
            w_copy(g, p, 13 + 2 * k, DELTA[k], 2, 1, 3, 128, 128).wait_recv()

    def project(g, k, acc_list, width):
        for p in (0, 1):
            acc = acc_list[p]
            w = bufs[g, p]

            def tile(i, _, acc=acc, w=w, p=p):
                r = pl.ds(pl.multiple_of((i % 3) * 256, 256), 256)
                c = pl.ds(pl.multiple_of((i // 3) * 256, 256), 256)
                total = None
                for v in range(4):
                    if p == 0:
                        j = ((z + DELTA[k]) % 4) * 4 + v
                    else:
                        j = v * 4 + (y + DELTA[k]) % 4
                    at = pl.ds(pl.multiple_of(j * KB, KB), KB)
                    part = mm(xs[r, at], w[at, c])
                    total = part if total is None else total + part
                if k == 0:
                    acc[r, c] = total
                else:
                    acc[r, c] += total
                return 0

            lax.fori_loop(0, 3 * (width // 256), tile, 0)

    send_first("q")
    go(x_copy(0, xi, 0, 48, right_x))
    go(x_copy(2, xi, 48, 48, left_x))
    go(x_copy(1, xi, 48, 48, right_x))
    go(x_copy(3, xi, 0, 48, left_x))
    go(x_copy(6, xi, 0, ROWS, to_sib))
    send_second("q", 0)

    wait_first("q")
    send_second("q", 1)
    send_second("q", 2)
    x_copy(0, xm, 0, 48, right_x).wait_recv()
    go(x_copy(4, xm, 0, 48, right_x))
    x_copy(2, xp, 48, 48, left_x).wait_recv()
    go(x_copy(5, xp, 48, 48, left_x))
    wait_first_halves("q")
    send_second("q", 3)
    wait_second("q", 0)
    x_copy(1, xm, 48, 48, right_x).wait_recv()
    go(x_copy(7, xm, 0, ROWS, to_sib))
    x_copy(3, xp, 0, 48, left_x).wait_recv()
    go(x_copy(8, xp, 0, ROWS, to_sib))
    wait_second("q", 1)
    wait_second("q", 2)
    send_first("c")
    x_copy(4, xf, 0, 48, right_x).wait_recv()
    x_copy(5, xf, 48, 48, left_x).wait_recv()
    go(x_copy(9, xf, 0, ROWS, to_sib))
    wait_second("q", 3)
    send_second("c", 0)
    for slot, src in ((6, xi), (7, xm), (8, xp), (9, xf)):
        x_copy(slot, src, 0, ROWS, to_sib, 1 - core).wait_recv()

    def rates(i, _):
        r = pl.ds(pl.multiple_of(i * 128, 128), 128)
        low = mm(xs[r, :], left[...]).astype(BF16)
        g = mm(low, right[...]) + offset[...]
        ls = jnp.minimum(g, 0.0) - jnp.log1p(jnp.exp(-jnp.abs(g)))
        rate[r, :] = ls * (1.0 / 16.0) + spikes[r, :]
        return 0

    lax.fori_loop(0, TOK // 128, rates, 0)

    wait_first("c")
    send_second("c", 1)
    send_second("c", 2)
    for k in range(4):
        wait_second_halves("q", k)
        project("q", k, (acc_a, acc_b), QA)
    wait_first_halves("c")
    send_second("c", 3)

    def store_qkv(i, _):
        r = pl.ds(pl.multiple_of(i * 64, 64), 64)
        qrows[r, :] = acc_a[r, 0:256].astype(BF16)
        krows[r, :] = acc_a[r, 256:512].astype(BF16)
        vrows[r, :] = acc_b[r, 0:512].astype(BF16)
        return 0

    lax.fori_loop(0, TOK // 64, store_qkv, 0)

    state[...] = jnp.zeros_like(state)
    prefix[...] = jnp.zeros_like(prefix)

    def attend(n, _):
        r = pl.ds(pl.multiple_of(n * BLOCK, BLOCK), BLOCK)
        row = lax.broadcasted_iota(jnp.int32, (BLOCK, BLOCK), 0)
        col = lax.broadcasted_iota(jnp.int32, (BLOCK, BLOCK), 1)
        causal = row >= col
        within = lax.dot_general(
            jnp.where(causal, 1.0, 0.0).astype(F32),
            rate[r, :],
            (((1,), (0,)), ((), ())),
            precision=HIGHEST,
            preferred_element_type=F32,
        )
        end = within[BLOCK - 1 : BLOCK, :]
        mid = end * 0.5
        q_s = qrows[r, :].astype(F32) * (KEY**-0.5) * jnp.exp(within - mid)
        k_s = krows[r, :].astype(F32) * jnp.exp(mid - within)
        e_mid = jnp.exp(mid)
        q_d = q_s * e_mid
        k_t = (k_s * e_mid).astype(BF16)
        e_end = jnp.exp(end)
        before = prefix[0:1, :]
        q_far[r, :] = (q_d * jnp.exp(before)).astype(BF16)
        prefix[0:1, :] = before + end
        q_d = q_d.astype(BF16)
        q_s = q_s.astype(BF16)
        k_s = k_s.astype(BF16)
        for h in range(2):
            kc = slice(h * KEY, (h + 1) * KEY)
            vc = slice(h * VAL, (h + 1) * VAL)
            v = vrows[r, vc]
            scores = jnp.where(causal, nt(q_s[:, kc], k_s[:, kc]), 0.0).astype(BF16)
            s = state[vc, :]
            inside[r, vc] = mm(scores, v) + nt(q_d[:, kc], s.astype(BF16))
            state[vc, :] = s * e_end[:, kc] + tn(v, k_t[:, kc])
        return 0

    lax.fori_loop(0, 6, attend, 0)
    wait_second("c", 0)
    lax.fori_loop(6, 12, attend, 0)
    wait_second("c", 1)

    def st_copy(phase, d, dst):
        i = phase * 3 + d - 1
        return (
            pltpu.make_async_remote_copy(
                src_ref=st_send.at[phase],
                dst_ref=st_recv.at[i],
                send_sem=s_send.at[0, i],
                recv_sem=s_recv.at[0, i],
                device_id=dst,
                device_id_type=MESH,
            ),
            pltpu.make_async_remote_copy(
                src_ref=dec_send.at[phase],
                dst_ref=dec_recv.at[i],
                send_sem=s_send.at[1, i],
                recv_sem=s_recv.at[1, i],
                device_id=dst,
                device_id_type=MESH,
            ),
        )

    own_decay = jnp.exp(prefix[0:1, :])
    st_send[0] = state[...].astype(BF16)
    dec_send[0] = jnp.broadcast_to(own_decay, (8, 2 * KEY))
    wait_second("c", 2)
    for d in (1, 2, 3):
        for c in st_copy(0, d, at_y(d)):
            go(c)
    wait_second("c", 3)
    wait_second_halves("c", 0)
    project("c", 0, (acc_a, acc_b), CA)
    for d in (1, 2, 3):
        for c in st_copy(0, d, at_y(d)):
            c.wait_recv()

    def fold(total, decay, i, use):
        dec = jnp.where(use, dec_recv[i][0:1, :], 1.0)
        out = []
        for h in range(2):
            kc = slice(h * KEY, (h + 1) * KEY)
            vc = slice(h * VAL, (h + 1) * VAL)
            got = jnp.where(use, st_recv[i, vc, :].astype(F32), 0.0)
            out.append(total[h] * dec[:, kc] + got)
        return out, decay * dec

    before_y = [jnp.zeros((VAL, KEY), F32) for _ in range(2)]
    decay_y = jnp.ones((1, 2 * KEY), F32)
    for d in (3, 2, 1):
        before_y, decay_y = fold(before_y, decay_y, d - 1, d <= y)
    total = [
        before_y[h] * own_decay[:, h * KEY : (h + 1) * KEY] + state[h * VAL : (h + 1) * VAL, :]
        for h in range(2)
    ]
    decay_row = decay_y * own_decay
    for h in range(2):
        state[h * VAL : (h + 1) * VAL, :] = before_y[h]
    for d in (3, 2, 1):
        total, decay_row = fold(total, decay_row, d - 1, d > y)
    for h in range(2):
        st_send[1, h * VAL : (h + 1) * VAL, :] = total[h].astype(BF16)
    dec_send[1] = jnp.broadcast_to(decay_row, (8, 2 * KEY))
    prefix[1:2, :] = decay_y
    wait_second_halves("c", 1)
    for d in (1, 2, 3):
        for c in st_copy(1, d, at_z(d)):
            go(c)
    project("c", 1, (acc_a, acc_b), CA)
    wait_second_halves("c", 2)
    project("c", 2, (acc_a, acc_b), CA)
    for d in (1, 2, 3):
        for c in st_copy(1, d, at_z(d)):
            c.wait_recv()
    before_z = [jnp.zeros((VAL, KEY), F32) for _ in range(2)]
    decay_z = jnp.ones((1, 2 * KEY), F32)
    for d in (3, 2, 1):
        before_z, decay_z = fold(before_z, decay_z, 3 + d - 1, d <= z)
    decay_y = prefix[1:2, :]
    for h in range(2):
        vc = slice(h * VAL, (h + 1) * VAL)
        state[vc, :] = before_z[h] * decay_y[:, h * KEY : (h + 1) * KEY] + state[vc, :]

    def finish(n, _):
        r = pl.ds(pl.multiple_of(n * 128, 128), 128)
        for h in range(2):
            kc = slice(h * KEY, (h + 1) * KEY)
            vc = slice(h * VAL, (h + 1) * VAL)
            a = inside[r, vc] + nt(q_far[r, kc], state[vc, :].astype(BF16))
            ms = jnp.mean(a * a, axis=-1, keepdims=True)
            attn_out[r, vc] = (a * lax.rsqrt(ms + EPS) * head_gain[h : h + 1, :]).astype(BF16)
        return 0

    lax.fori_loop(0, TOK // 128, finish, 0)

    wait_second_halves("c", 3)
    project("c", 3, (acc_a, acc_b), CA)

    def gate(i, _):
        r = pl.ds(pl.multiple_of(i * 64, 64), 64)
        o = pl.ds(pl.multiple_of(i * 64 + 8, 8), 64)
        gated[o, 0:256] = (
            (acc_a[r, 512:768].astype(BF16).astype(F32) * acc_b[r, 256:512].astype(BF16).astype(F32))
            .astype(BF16)
            .astype(F32)
        )
        gated[o, 256:512] = (
            (acc_b[r, 0:256].astype(BF16).astype(F32) * acc_b[r, 512:768].astype(BF16).astype(F32))
            .astype(BF16)
            .astype(F32)
        )
        return 0

    lax.fori_loop(0, TOK // 64, gate, 0)
    halo = pltpu.make_async_remote_copy(
        src_ref=gated.at[pl.ds(TOK, 8), :],
        dst_ref=gated.at[pl.ds(0, 8), :],
        send_sem=h_sem.at[0],
        recv_sem=h_sem.at[1],
        device_id=to_next,
        device_id_type=MESH,
    )
    go(halo)

    def conv(first, i):
        r0 = i * 64
        block = gated[pl.ds(pl.multiple_of(r0, 8), 72), :]
        if first:
            keep = jnp.where(sp == 0, 0.0, 1.0)
            rim = lax.broadcasted_iota(jnp.int32, (72, 1), 0) < 8
            block = jnp.where(rim, block * keep, block)
        one = pltpu.roll(block, 1, 0)[8:, :]
        two = pltpu.roll(block, 2, 0)[8:, :]
        s = taps[0:1, :] * two + taps[1:2, :] * one + taps[2:3, :] * block[8:, :]
        r = pl.ds(pl.multiple_of(r0, 64), 64)
        outer = acc_a[r, 0:512].astype(BF16).astype(F32)
        conv_out[r, :] = (s * outer).astype(BF16)

    def conv_step(i, _):
        conv(False, i)
        return 0

    lax.fori_loop(1, TOK // 64, conv_step, 0)
    halo.wait_recv()
    conv(True, 0)
    for c in started:
        c.wait_send()


def front(*args):
    any_ = pl.BlockSpec(memory_space=pl.ANY)
    vmem = pl.BlockSpec(memory_space=pltpu.VMEM)
    dma = pltpu.SemaphoreType.DMA
    return pl.pallas_call(
        front_kernel,
        out_shape=(
            jax.ShapeDtypeStruct((TOK, 2 * VAL), BF16),
            jax.ShapeDtypeStruct((TOK, 512), BF16),
        ),
        in_specs=[any_, vmem] + [any_] * 6 + [vmem] * 6,
        out_specs=(vmem, vmem),
        scratch_shapes=[
            pltpu.VMEM((TOK, MODEL), BF16),
            pltpu.VMEM((MODEL, QA), BF16),
            pltpu.VMEM((MODEL, QA), BF16),
            pltpu.VMEM((MODEL, CA), BF16),
            pltpu.VMEM((MODEL, CA), BF16),
            pltpu.VMEM((TOK, CA), F32),
            pltpu.VMEM((TOK, CA), F32),
            pltpu.VMEM((TOK, 2 * KEY), BF16),
            pltpu.VMEM((TOK, 2 * KEY), BF16),
            pltpu.VMEM((TOK, 2 * VAL), BF16),
            pltpu.VMEM((TOK, 2 * KEY), F32),
            pltpu.VMEM((TOK, 2 * VAL), F32),
            pltpu.VMEM((TOK, 2 * KEY), BF16),
            pltpu.VMEM((2 * VAL, KEY), F32),
            pltpu.VMEM((8, 2 * KEY), F32),
            pltpu.VMEM((2, 2 * VAL, KEY), BF16),
            pltpu.VMEM((2, 8, 2 * KEY), F32),
            pltpu.VMEM((6, 2 * VAL, KEY), BF16),
            pltpu.VMEM((6, 8, 2 * KEY), F32),
            pltpu.VMEM((TOK + 8, 512), F32),
            dma((8,)),
            dma((4, 20)),
            dma((4, 20)),
            dma((10,)),
            dma((10,)),
            dma((2, 6)),
            dma((2, 6)),
            dma((2,)),
        ],
        compiler_params=pltpu.CompilerParams(
            collective_id=0, has_side_effects=True, vmem_limit_bytes=60 * 1024 * 1024
        ),
        name="front",
    )(*args)


CHUNKS = 8
CW = MODEL // CHUNKS


def back_kernel(
    attn,
    conv,
    w_a,
    w_c,
    out,
    mix,
    w,
    full,
    sib_send,
    sib_recv,
    far_send,
    far_recv,
    near_send,
    near_recv,
    load_sem,
    ss,
    sr,
    fs,
    fr,
    ns,
    nr,
):
    t = lax.axis_index("tp")
    core = t % 2
    xi = t // 2

    def at_x(d):
        return {"tp": ((xi + d) % 4) * 2 + core}

    to_sib = {"tp": xi * 2 + (1 - core)}
    loads = [
        pltpu.make_async_copy(attn, mix.at[:, 0:512], load_sem.at[0]),
        pltpu.make_async_copy(conv, mix.at[:, 512:1024], load_sem.at[1]),
    ]
    for c in range(CHUNKS):
        cols = pl.ds(c * CW, CW)
        loads.append(pltpu.make_async_copy(w_a.at[:, cols], w.at[c, 0:512, :], load_sem.at[2 + 2 * c]))
        loads.append(pltpu.make_async_copy(w_c.at[:, cols], w.at[c, 512:1024, :], load_sem.at[3 + 2 * c]))
    for c in loads:
        c.start()
    barrier = pltpu.get_barrier_semaphore()
    peers = [at_x(1), at_x(3), to_sib]
    for p in peers:
        pl.semaphore_signal(barrier, inc=1, device_id=p, device_id_type=MESH)
    loads[0].wait()
    loads[1].wait()
    pl.semaphore_wait(barrier, len(peers))

    def sib_copy(c):
        return pltpu.make_async_remote_copy(
            src_ref=sib_send.at[c],
            dst_ref=sib_recv.at[c],
            send_sem=ss.at[c],
            recv_sem=sr.at[c],
            device_id=to_sib,
            device_id_type=MESH,
        )

    def far_copy(c, side):
        return pltpu.make_async_remote_copy(
            src_ref=far_send.at[c, side],
            dst_ref=far_recv.at[c, side],
            send_sem=fs.at[c, side],
            recv_sem=fr.at[c, side],
            device_id=at_x(1 if side == 0 else 3),
            device_id_type=MESH,
        )

    def near_copy(c, side):
        return pltpu.make_async_remote_copy(
            src_ref=near_send.at[c, side],
            dst_ref=near_recv.at[c, side],
            send_sem=ns.at[c, side],
            recv_sem=nr.at[c, side],
            device_id=at_x(1 if side == 0 else 3),
            device_id_type=MESH,
        )

    def group(d, mine):
        g = ((xi + d) % 4) * 2 + (core if mine else 1 - core)
        return pl.multiple_of(g * ROWS, 32)

    def stage_a(c):
        loads[2 + 2 * c].wait()
        loads[3 + 2 * c].wait()

        def tile(i, _):
            r = pl.ds(pl.multiple_of((i % 3) * 256, 256), 256)
            k = pl.ds(pl.multiple_of((i // 3) * 256, 256), 256)
            full[c % 4, r, k] = mm(mix[r, :], w[c, :, k])
            return 0

        lax.fori_loop(0, 3 * (CW // 256), tile, 0)
        for d in range(4):
            sib_send[c, d * ROWS : (d + 1) * ROWS, :] = full[c % 4, pl.ds(group(d, False), ROWS), :].astype(BF16)
        sib_copy(c).start()

    def pair(c, d, r0, rows):
        here = full[c % 4, pl.ds(pl.multiple_of(group(d, True) + r0, 16), rows), :]
        return here + sib_recv[c, d * ROWS + r0 : d * ROWS + r0 + rows, :].astype(F32)

    def stage_b(c):
        sib_copy(c).wait_recv()
        far_send[c, 0] = pair(c, 2, 0, 48).astype(BF16)
        far_send[c, 1] = pair(c, 2, 48, 48).astype(BF16)
        far_copy(c, 0).start()
        far_copy(c, 1).start()

    def stage_c(c):
        far_copy(c, 0).wait_recv()
        near_send[c, 0, 0:48, :] = (pair(c, 1, 0, 48) + far_recv[c, 0].astype(F32)).astype(BF16)
        near_send[c, 0, 48:96, :] = pair(c, 1, 48, 48).astype(BF16)
        near_copy(c, 0).start()
        far_copy(c, 1).wait_recv()
        near_send[c, 1, 0:48, :] = pair(c, 3, 0, 48).astype(BF16)
        near_send[c, 1, 48:96, :] = (pair(c, 3, 48, 48) + far_recv[c, 1].astype(F32)).astype(BF16)
        near_copy(c, 1).start()

    def stage_d(c):
        near_copy(c, 0).wait_recv()
        near_copy(c, 1).wait_recv()
        total = pair(c, 0, 0, ROWS) + near_recv[c, 0].astype(F32) + near_recv[c, 1].astype(F32)
        out[:, c * CW : (c + 1) * CW] = total.astype(BF16)

    for i in range(CHUNKS + 3):
        if i < CHUNKS:
            stage_a(i)
        if 0 <= i - 1 < CHUNKS:
            stage_b(i - 1)
        if 0 <= i - 2 < CHUNKS:
            stage_c(i - 2)
        if 0 <= i - 3 < CHUNKS:
            stage_d(i - 3)
    for c in range(CHUNKS):
        sib_copy(c).wait_send()
        for side in (0, 1):
            far_copy(c, side).wait_send()
            near_copy(c, side).wait_send()


def back(*args):
    any_ = pl.BlockSpec(memory_space=pl.ANY)
    vmem = pl.BlockSpec(memory_space=pltpu.VMEM)
    dma = pltpu.SemaphoreType.DMA
    return pl.pallas_call(
        back_kernel,
        out_shape=jax.ShapeDtypeStruct((ROWS, MODEL), BF16),
        in_specs=[any_] * 4,
        out_specs=vmem,
        scratch_shapes=[
            pltpu.VMEM((TOK, 1024), BF16),
            pltpu.VMEM((CHUNKS, 1024, CW), BF16),
            pltpu.VMEM((4, TOK, CW), F32),
            pltpu.VMEM((CHUNKS, 4 * ROWS, CW), BF16),
            pltpu.VMEM((CHUNKS, 4 * ROWS, CW), BF16),
            pltpu.VMEM((CHUNKS, 2, 48, CW), BF16),
            pltpu.VMEM((CHUNKS, 2, 48, CW), BF16),
            pltpu.VMEM((CHUNKS, 2, ROWS, CW), BF16),
            pltpu.VMEM((CHUNKS, 2, ROWS, CW), BF16),
            dma((2 + 2 * CHUNKS,)),
            dma((CHUNKS,)),
            dma((CHUNKS,)),
            dma((CHUNKS, 2)),
            dma((CHUNKS, 2)),
            dma((CHUNKS, 2)),
            dma((CHUNKS, 2)),
        ],
        compiler_params=pltpu.CompilerParams(
            collective_id=1, has_side_effects=True, vmem_limit_bytes=60 * 1024 * 1024
        ),
        name="back",
    )(*args)


def body(
    hidden_activations,
    entry_rescale_vector,
    probe_matrix,
    lookup_address_matrix,
    payload_matrix,
    postfilter_switch_matrix,
    prefilter_switch_matrix,
    filter_source_matrix,
    forget_left_factor,
    forget_right_factor,
    forget_offset_per_feature,
    forget_spike_additions,
    subspace_rescale_vector,
    depthwise_filter_taps,
    mixer_result_matrix,
    filter_result_matrix,
):
    spikes = jnp.repeat(jnp.transpose(forget_spike_additions), KEY, axis=1)
    mixed_attn, mixed_conv = front(
        hidden_activations,
        entry_rescale_vector.astype(F32)[None, :],
        probe_matrix,
        lookup_address_matrix,
        payload_matrix,
        postfilter_switch_matrix,
        prefilter_switch_matrix,
        filter_source_matrix,
        forget_left_factor,
        forget_right_factor,
        forget_offset_per_feature[None, :],
        spikes,
        subspace_rescale_vector.astype(F32),
        depthwise_filter_taps.astype(F32),
    )
    return back(mixed_attn, mixed_conv, mixer_result_matrix, filter_result_matrix)


def solution(mesh):
    split = Mesh(mesh.devices.reshape(4, 4, mesh.shape["tp"]), ("sp_0", "sp_1", "tp"))
    in_specs = (
        P(SP_TP, None),
        P(),
        P(SP, "tp"),
        P(SP, "tp"),
        P(SP, "tp"),
        P(SP, "tp"),
        P(SP, "tp"),
        P(SP, "tp"),
        P(),
        P(None, "tp"),
        P("tp"),
        P("tp", SP),
        P("tp", None),
        P(None, "tp"),
        P("tp", None),
        P("tp", None),
    )
    out_specs = P(SP_TP, None)
    return jax.shard_map(body, mesh=split, in_specs=in_specs, out_specs=out_specs, check_vma=False)
```

```python
import jax
import jax.numpy as jnp
from jax import lax
from jax.experimental import pallas as pl
from jax.experimental.pallas import tpu as pltpu
from jax.sharding import Mesh
from jax.sharding import PartitionSpec as P

MESH = pl.DeviceIdType.MESH
SP = ("sp_0", "sp_1")
SP_TP = ("sp_0", "sp_1", "tp")
F32 = jnp.float32
BF16 = jnp.bfloat16
HIGHEST = lax.Precision.HIGHEST

BLOCK = 64
ROWS = 96
TOK = 768
MODEL = 4096
KB = 256
LATE = 128
EARLY = 512 - LATE
MIX = 512 + EARLY
CHUNKS = 8
CW = MODEL // CHUNKS
KEY, VAL = 128, 256
EPS = 1e-06
DELTA = (0, 3, 1, 2)


def nt(a, b):
    return lax.dot_general(a, b, (((1,), (1,)), ((), ())), preferred_element_type=F32)


def tn(a, b):
    return lax.dot_general(a, b, (((0,), (0,)), ((), ())), preferred_element_type=F32)


def mm(a, b):
    return jnp.dot(a, b, preferred_element_type=F32)


def plan(p):
    p.first("q")
    p.ring_start("x")
    p.second("q", 0)
    p.wfirst("q")
    p.second("q", 1)
    p.ring_relay("x")
    p.wfh("q")
    p.second("q", 2)
    p.second("q", 3)
    p.wsecond("q", 0)
    p.ring_mid("x")
    p.ring_start("f")
    p.wsecond("q", 1)
    p.ring_far("x")
    p.wsecond("q", 2)
    p.first("c")
    p.wsecond("q", 3)
    p.ring_end("x")
    p.rates()
    p.second("c", 0)
    p.wsh("q", 0)
    p.project("q", 0)
    p.wsh("q", 1)
    p.project("q", 1)
    p.wfirst("c")
    p.second("c", 1)
    p.wsh("q", 2)
    p.project("q", 2)
    p.wsh("q", 3)
    p.project("q", 3)
    p.key_state()
    p.state(0)
    p.ring_relay("f")
    p.wfh("c")
    p.wsecond("c", 0)
    p.second("c", 2)
    p.attend(0, 6)
    p.rstate(0)
    p.second("c", 3)
    p.wsecond("c", 1)
    p.ring_mid("f")
    p.attend(6, 12)
    p.wstate(0)
    p.fold_y()
    p.state(1)
    p.load_out()
    p.wsh("c", 0)
    p.project("c", 0)
    p.wsecond("c", 2)
    p.rstate(1)
    p.wsecond("c", 3)
    p.wsh("c", 1)
    p.project("c", 1)
    p.first("d")
    p.ring_far("f")
    p.wstate(1)
    p.fold_z()
    p.second("d", 0)
    p.wsh("c", 2)
    p.project("c", 2)
    p.wfirst("d")
    p.second("d", 1)
    p.second("d", 2)
    p.wsh("c", 3)
    p.project("c", 3)
    p.wfh("d")
    p.second("d", 3)
    p.conv("c")

    def late(k):
        p.wsh("d", k)
        p.project("d", k)

    def finish_late():
        p.conv("d")
        p.exchange()

    extra = {
        0: lambda: p.wsecond("d", 0),
        1: lambda: p.wsecond("d", 1),
        2: lambda: (p.wsecond("d", 2), p.wsecond("d", 3)),
        3: lambda: late(0),
        4: lambda: late(1),
        5: lambda: late(2),
        6: lambda: (late(3), finish_late()),
        8: lambda: p.ring_end("f"),
    }
    for i in range(CHUNKS + 3):
        if i < CHUNKS:
            p.pair_products(i)
        if 0 <= i - 1 < CHUNKS:
            p.far(i - 1)
        if 0 <= i - 2 < CHUNKS:
            p.near(i - 2)
        if i in extra:
            extra[i]()
        if 0 <= i - 3 < CHUNKS:
            p.gather(i - 3)
    p.last()


def layer_kernel(
    x_in,
    gain,
    w_q,
    w_k,
    w_v,
    w_out,
    w_in,
    w_src,
    left,
    right,
    offset,
    spikes,
    head_gain,
    taps,
    w_a,
    w_c,
    out,
    xs,
    qa,
    qb,
    ca,
    cb,
    da,
    db,
    wf,
    acc_a,
    acc_b,
    acc_da,
    acc_db,
    qrows,
    krows,
    vrows,
    within,
    tail,
    spk,
    inside,
    q_far,
    state,
    prefix,
    st_send,
    dec_send,
    st_recv,
    dec_recv,
    gated_c,
    gated_d,
    mix,
    late_mix,
    late_recv,
    own,
    sib_send,
    sib_recv,
    far_send,
    far_recv,
    near_send,
    near_recv,
    load_sem,
    out_sem,
    w_send,
    w_recv,
    x_send,
    x_recv,
    s_send,
    s_recv,
    h_send,
    h_recv,
    e_send,
    e_recv,
    ss,
    sr,
    fs,
    fr,
    ns,
    nr,
):
    z = lax.axis_index("sp_0")
    y = lax.axis_index("sp_1")
    t = lax.axis_index("tp")
    core = t % 2
    xi = t // 2
    sp = z * 4 + y
    sp_next = (sp + 1) % 16
    sp_prev = (sp + 15) % 16
    to_next = {"sp_0": sp_next // 4, "sp_1": sp_next % 4}
    to_prev = {"sp_0": sp_prev // 4, "sp_1": sp_prev % 4}
    to_sib = {"tp": xi * 2 + (1 - core)}

    def at_z(d):
        return {"sp_0": (z + d) % 4}

    def at_y(d):
        return {"sp_1": (y + d) % 4}

    def at_x(d):
        return {"tp": ((xi + d) % 4) * 2 + core}

    def remote(ref, dst, sems, at, to):
        return pltpu.make_async_remote_copy(
            src_ref=ref,
            dst_ref=dst,
            send_sem=sems[0].at[at],
            recv_sem=sems[1].at[at],
            device_id=to,
            device_id_type=MESH,
        )

    own0 = pl.ds(pl.multiple_of(sp * KB, KB), KB)
    own1 = pl.ds(pl.multiple_of((y * 4 + z) * KB, KB), KB)
    own_rows = pl.multiple_of(t * ROWS, 32)
    loads = [
        (x_in, xs.at[pl.ds(own_rows, ROWS), :]),
        (w_q, qa.at[own0, 0:256]),
        (w_k, qa.at[own0, 256:512]),
        (w_v, qb.at[own1, :]),
        (w_in.at[:, 256:384], ca.at[own0, 0:128]),
        (w_src.at[:, 0:384], ca.at[own0, 128:512]),
        (w_out.at[:, 0:384], cb.at[own1, 0:384]),
        (w_in.at[:, 0:256], cb.at[own1, 384:640]),
        (w_in.at[:, 384:512], da.at[own0, 0:128]),
        (w_src.at[:, 384:512], da.at[own0, 128:256]),
        (w_out.at[:, 384:512], db.at[own1, :]),
        (w_c.at[EARLY:512, :], wf.at[pl.ds(pl.multiple_of(t * LATE, LATE), LATE), :]),
    ]
    loads = [pltpu.make_async_copy(a, b, load_sem.at[i]) for i, (a, b) in enumerate(loads)]
    for c in loads:
        c.start()

    barrier = pltpu.get_barrier_semaphore()
    peers = [at_z(1), at_z(3), at_y(1), at_y(3), to_next, to_prev] + [{"tp": (t + d) % 8} for d in range(1, 8)]
    for p in peers:
        pl.semaphore_signal(barrier, inc=1, device_id=p, device_id_type=MESH)

    loads[0].wait()

    def norm_rows(i, _):
        r = pl.ds(pl.multiple_of(own_rows + i * 16, 16), 16)
        v = xs[r, :].astype(F32)
        inv = lax.rsqrt(jnp.mean(v * v, axis=-1, keepdims=True) + EPS)
        g = gain[...].astype(F32)
        for c in range(32):
            k = slice(c * 128, (c + 1) * 128)
            xs[r, k] = (v[:, k] * inv * g[c : c + 1, :]).astype(BF16)
        return 0

    lax.fori_loop(0, ROWS // 16, norm_rows, 0)
    spk[...] = jnp.zeros_like(spk)
    spk[0:2, :] = spikes[...]
    for c in loads[1:]:
        c.wait()
    pl.semaphore_wait(barrier, len(peers))

    started = []
    started_q = []

    def go(c, group=None):
        c.start()
        (started_q if group == "q" else started).append(c)

    bufs = {"q": (qa, qb), "c": (ca, cb), "d": (da, db)}
    accs = {"q": (acc_a, acc_b.at[:, 0:512]), "c": (acc_a, acc_b), "d": (acc_da, acc_db)}
    base = {"q": 0, "c": 2, "d": 4}
    rings = {"x": (xs, ROWS, 0), "f": (wf, LATE, 10)}
    xm, xp, xf = (xi + 3) % 4, (xi + 1) % 4, (xi + 2) % 4

    def w_copy(g, path, slot, du, dv, axis, step, row=0, rows=KB):
        u0, v0 = (z, y) if path == 0 else (y, z)
        j = ((u0 + du) % 4) * 4 + (v0 + dv) % 4
        ref = bufs[g][path].at[pl.ds(pl.multiple_of(j * KB + row, 128), rows), :]
        to = at_z(step) if (axis == 0) == (path == 0) else at_y(step)
        return remote(ref, ref, (w_send, w_recv), (base[g] + path, slot), to)

    def ring_copy(n, slot, x_from, top, halves, to, c=None):
        buf, rows, first = rings[n]
        half = rows // 2
        at = (x_from * 2 + (core if c is None else c)) * rows + (0 if top else half)
        ref = buf.at[pl.ds(pl.multiple_of(at, 16), half * halves), :]
        return remote(ref, ref, (x_send, x_recv), first + slot, to)

    right_x, left_x = at_x(1), at_x(3)

    def st_copy(ph, slot):
        to = (at_y if ph == 0 else at_z)(1 if slot % 2 == 0 else 3)
        i = ph * 3
        if slot < 2:
            a, b = st_send.at[ph], st_recv.at[i + 2 * slot]
        else:
            half = pl.ds((slot - 2) * VAL, VAL)
            a, b = st_recv.at[i + 2 * (slot - 2), half, :], st_recv.at[i + 1, half, :]
        return remote(a, b, (s_send, s_recv), ph * 8 + slot, to)

    def dec_copy(ph, slot):
        to = (at_y if ph == 0 else at_z)(1 if slot != 1 else 3)
        i = ph * 3
        if slot < 2:
            a, b = dec_send.at[ph], dec_recv.at[i + 2 * slot]
        else:
            a, b = dec_recv.at[i], dec_recv.at[i + 1]
        return remote(a, b, (s_send, s_recv), ph * 8 + 4 + slot, to)

    def halo_copy(g):
        buf = gated_c if g == "c" else gated_d
        i = 0 if g == "c" else 1
        return remote(buf.at[pl.ds(TOK, 8), :], buf.at[pl.ds(0, 8), :], (h_send, h_recv), i, to_next)

    def sib_copy(c):
        return remote(sib_send.at[c % 2], sib_recv.at[c], (ss, sr), c, to_sib)

    def far_copy(c, side):
        return remote(far_send.at[c, side], far_recv.at[c, side], (fs, fr), (c, side), right_x if side == 0 else left_x)

    def near_copy(c, side):
        return remote(near_send.at[c, side], near_recv.at[c, side], (ns, nr), (c, side), right_x if side == 0 else left_x)

    def late_copy(d, sending):
        g = (t + d) % 8
        me = t if sending else (t + 8 - d) % 8
        src = late_mix.at[pl.ds(pl.multiple_of(g * ROWS, 32), ROWS), :]
        return remote(src, late_recv.at[me], (e_send, e_recv), d - 1, {"tp": g})

    def out_block(i):
        return (qa if i < CHUNKS // 2 else qb).at[pl.ds((i % (CHUNKS // 2)) * MIX, MIX), :]

    def out_loads(i):
        cols = pl.ds(i * CW, CW)
        w = out_block(i)
        return (
            pltpu.make_async_copy(w_a.at[:, cols], w.at[0:512, :], out_sem.at[2 * i]),
            pltpu.make_async_copy(w_c.at[0:EARLY, cols], w.at[512:MIX, :], out_sem.at[2 * i + 1]),
        )

    def head(h):
        return slice(h * KEY, (h + 1) * KEY), slice(h * VAL, (h + 1) * VAL)

    class Device:
        def first(self, g):
            for p in (0, 1):
                go(w_copy(g, p, 0, 0, 0, 0, 1), g)
                go(w_copy(g, p, 1, 0, 0, 0, 3), g)

        def wfirst(self, g):
            for p in (0, 1):
                w_copy(g, p, 0, 3, 0, 0, 1).wait_recv()
                go(w_copy(g, p, 2, 3, 0, 0, 1, 0, 128), g)
                w_copy(g, p, 1, 1, 0, 0, 3).wait_recv()
                go(w_copy(g, p, 3, 1, 0, 0, 3, 128, 128), g)

        def wfh(self, g):
            for p in (0, 1):
                w_copy(g, p, 2, 2, 0, 0, 1, 0, 128).wait_recv()
                w_copy(g, p, 3, 2, 0, 0, 3, 128, 128).wait_recv()

        def second(self, g, k):
            for p in (0, 1):
                go(w_copy(g, p, 4 + 2 * k, DELTA[k], 0, 1, 1), g)
                go(w_copy(g, p, 5 + 2 * k, DELTA[k], 0, 1, 3), g)

        def wsecond(self, g, k):
            for p in (0, 1):
                w_copy(g, p, 4 + 2 * k, DELTA[k], 3, 1, 1).wait_recv()
                go(w_copy(g, p, 12 + 2 * k, DELTA[k], 3, 1, 1, 0, 128), g)
                w_copy(g, p, 5 + 2 * k, DELTA[k], 1, 1, 3).wait_recv()
                go(w_copy(g, p, 13 + 2 * k, DELTA[k], 1, 1, 3, 128, 128), g)

        def wsh(self, g, k):
            for p in (0, 1):
                w_copy(g, p, 12 + 2 * k, DELTA[k], 2, 1, 1, 0, 128).wait_recv()
                w_copy(g, p, 13 + 2 * k, DELTA[k], 2, 1, 3, 128, 128).wait_recv()

        def ring_start(self, n):
            go(ring_copy(n, 0, xi, True, 1, right_x))
            go(ring_copy(n, 2, xi, False, 1, left_x))
            go(ring_copy(n, 1, xi, False, 1, right_x))
            go(ring_copy(n, 3, xi, True, 1, left_x))
            go(ring_copy(n, 6, xi, True, 2, to_sib))

        def ring_relay(self, n):
            ring_copy(n, 0, xm, True, 1, right_x).wait_recv()
            go(ring_copy(n, 4, xm, True, 1, right_x))
            ring_copy(n, 2, xp, False, 1, left_x).wait_recv()
            go(ring_copy(n, 5, xp, False, 1, left_x))

        def ring_mid(self, n):
            ring_copy(n, 1, xm, False, 1, right_x).wait_recv()
            go(ring_copy(n, 7, xm, True, 2, to_sib))
            ring_copy(n, 3, xp, True, 1, left_x).wait_recv()
            go(ring_copy(n, 8, xp, True, 2, to_sib))

        def ring_far(self, n):
            ring_copy(n, 4, xf, True, 1, right_x).wait_recv()
            ring_copy(n, 5, xf, False, 1, left_x).wait_recv()
            go(ring_copy(n, 9, xf, True, 2, to_sib))

        def ring_end(self, n):
            for slot, src in ((6, xi), (7, xm), (8, xp), (9, xf)):
                ring_copy(n, slot, src, True, 2, to_sib, 1 - core).wait_recv()

        def rates(self):
            lane_head = lax.broadcasted_iota(jnp.int32, (8, 2 * KEY), 1) // KEY
            pick = jnp.where(lax.broadcasted_iota(jnp.int32, (8, 2 * KEY), 0) == lane_head, 1.0, 0.0).astype(F32)
            row = lax.broadcasted_iota(jnp.int32, (128, 128), 0)
            col = lax.broadcasted_iota(jnp.int32, (128, 128), 1)
            low_tri = jnp.where((row >= col) & (row // BLOCK == col // BLOCK), 1.0, 0.0).astype(F32)

            def step(i, _):
                r = pl.ds(pl.multiple_of(i * 128, 128), 128)
                low = nt(xs[r, :], left[...]).astype(BF16)
                g = mm(low, right[...]) + offset[...]
                ls = jnp.minimum(g, 0.0) - jnp.log1p(jnp.exp(-jnp.abs(g)))
                spike = lax.dot_general(
                    spk[:, r], pick, (((0,), (0,)), ((), ())), precision=HIGHEST, preferred_element_type=F32
                )
                within[r, :] = jnp.dot(
                    low_tri, ls * (1.0 / 16.0) + spike, precision=HIGHEST, preferred_element_type=F32
                )
                return 0

            lax.fori_loop(0, TOK // 128, step, 0)
            prefix[0:1, :] = jnp.zeros((1, 2 * KEY), F32)

            def back(i, _):
                n = TOK // BLOCK - 1 - i
                w = within[pl.ds(pl.multiple_of(n * BLOCK, BLOCK), BLOCK), :]
                end = w[BLOCK - 1 : BLOCK, :]
                later = prefix[0:1, :]
                tail[pl.ds(pl.multiple_of(n * BLOCK, BLOCK), BLOCK), :] = jnp.exp(end - w + later)
                prefix[0:1, :] = later + end
                return 0

            lax.fori_loop(0, TOK // BLOCK, back, 0)
            dec_send[0] = jnp.broadcast_to(jnp.exp(prefix[0:1, :]), (8, 2 * KEY))

        def project(self, g, k):
            for p in (0, 1):
                w, acc = bufs[g][p], accs[g][p]
                u = ((z if p == 0 else y) + DELTA[k]) % 4
                if p == 0:
                    lhs = xs[:, pl.ds(pl.multiple_of(u * 1024, 1024), 1024)]
                else:
                    lhs = jnp.concatenate(
                        [xs[:, pl.ds(pl.multiple_of((v * 4 + u) * KB, KB), KB)] for v in range(4)], axis=1
                    )
                part = mm(lhs, w[pl.ds(pl.multiple_of(u * 1024, 1024), 1024), :])
                if k == 0:
                    acc[...] = part
                else:
                    acc[...] += part

        def key_state(self):
            def step(i, _):
                r = pl.ds(pl.multiple_of(i * 64, 64), 64)
                qrows[r, :] = acc_a[r, 0:256].astype(BF16)
                krows[r, :] = acc_a[r, 256:512].astype(BF16)
                vrows[r, :] = acc_b[r, 0:512].astype(BF16)
                return 0

            lax.fori_loop(0, TOK // 64, step, 0)
            k_tail = (krows[...].astype(F32) * tail[...]).astype(BF16)
            for h in range(2):
                kc, vc = head(h)
                s = tn(vrows[:, vc], k_tail[:, kc])
                st_send[0, vc, :] = s.astype(BF16)
            state[...] = jnp.zeros_like(state)
            prefix[0:1, :] = jnp.zeros((1, 2 * KEY), F32)

        def state(self, ph):
            for slot in (0, 1):
                go(st_copy(ph, slot))
                go(dec_copy(ph, slot))

        def rstate(self, ph):
            for slot in (0, 1):
                st_copy(ph, slot).wait_recv()
                dec_copy(ph, slot).wait_recv()
                go(st_copy(ph, slot + 2))
            go(dec_copy(ph, 2))

        def wstate(self, ph):
            st_copy(ph, 2).wait_recv()
            st_copy(ph, 3).wait_recv()
            dec_copy(ph, 2).wait_recv()

        def attend(self, lo, hi):
            def step(n, _):
                r = pl.ds(pl.multiple_of(n * BLOCK, BLOCK), BLOCK)
                row = lax.broadcasted_iota(jnp.int32, (BLOCK, BLOCK), 0)
                col = lax.broadcasted_iota(jnp.int32, (BLOCK, BLOCK), 1)
                causal = row >= col
                w = within[r, :]
                end = w[BLOCK - 1 : BLOCK, :]
                mid = end * 0.5
                q_s = qrows[r, :].astype(F32) * (KEY**-0.5) * jnp.exp(w - mid)
                k_s = krows[r, :].astype(F32) * jnp.exp(mid - w)
                e_mid = jnp.exp(mid)
                q_d = q_s * e_mid
                k_t = (k_s * e_mid).astype(BF16)
                e_end = jnp.exp(end)
                before = prefix[0:1, :]
                q_far[r, :] = (q_d * jnp.exp(before)).astype(BF16)
                prefix[0:1, :] = before + end
                q_d = q_d.astype(BF16)
                q_s = q_s.astype(BF16)
                k_s = k_s.astype(BF16)
                for h in range(2):
                    kc, vc = head(h)
                    v = vrows[r, vc]
                    scores = jnp.where(causal, nt(q_s[:, kc], k_s[:, kc]), 0.0).astype(BF16)
                    s = state[vc, :]
                    inside[r, vc] = mm(scores, v) + nt(q_d[:, kc], s.astype(BF16))
                    state[vc, :] = s * e_end[:, kc] + tn(v, k_t[:, kc])
                return 0

            lax.fori_loop(lo, hi, step, 0)

        def fold(self, total, decay, i, use):
            dec = jnp.where(use, dec_recv[i][0:1, :], 1.0)
            out_ = []
            for h in range(2):
                kc, vc = head(h)
                got = jnp.where(use, st_recv[i, vc, :].astype(F32), 0.0)
                out_.append(total[h] * dec[:, kc] + got)
            return out_, decay * dec

        def fold_y(self):
            own_decay = dec_send[0][0:1, :]
            total = [jnp.zeros((VAL, KEY), F32) for _ in range(2)]
            decay = jnp.ones((1, 2 * KEY), F32)
            for d in (3, 2, 1):
                total, decay = self.fold(total, decay, d - 1, d <= y)
            prefix[1:2, :] = decay
            for h in range(2):
                kc, vc = head(h)
                state[vc, :] = total[h]
                total[h] = total[h] * own_decay[:, kc] + st_send[0, vc, :].astype(F32)
            decay = decay * own_decay
            for d in (3, 2, 1):
                total, decay = self.fold(total, decay, d - 1, d > y)
            for h in range(2):
                kc, vc = head(h)
                st_send[1, vc, :] = total[h].astype(BF16)
            dec_send[1] = jnp.broadcast_to(decay, (8, 2 * KEY))

        def fold_z(self):
            total = [jnp.zeros((VAL, KEY), F32) for _ in range(2)]
            decay = jnp.ones((1, 2 * KEY), F32)
            for d in (3, 2, 1):
                total, decay = self.fold(total, decay, 3 + d - 1, d <= z)
            decay = prefix[1:2, :]
            for h in range(2):
                kc, vc = head(h)
                state[vc, :] = total[h] * decay[:, kc] + state[vc, :]
            hg = head_gain[...].astype(F32)

            def finish(g, _):
                r = pl.ds(pl.multiple_of(g * ROWS, 32), ROWS)
                to = self.place(g)
                for h in range(2):
                    kc, vc = head(h)
                    a = inside[r, vc] + nt(q_far[r, kc], state[vc, :].astype(BF16))
                    ms = jnp.mean(a * a, axis=-1, keepdims=True)
                    mix[to, vc] = (a * lax.rsqrt(ms + EPS) * hg[h : h + 1, :]).astype(BF16)
                return 0

            lax.fori_loop(0, 8, finish, 0)

        def place(self, g):
            mine = 1 - (g + core) % 2
            d = (g // 2 + 4 - xi) % 4
            return pl.ds(pl.multiple_of((mine * 4 + d) * ROWS, 32), ROWS)

        def conv(self, g):
            gated = gated_c if g == "c" else gated_d
            lanes = slice(0, EARLY) if g == "c" else slice(EARLY, 512)

            def rnd(v):
                return v.astype(BF16).astype(F32)

            def gate(i, _):
                r = pl.ds(pl.multiple_of(i * 64, 64), 64)
                o = pl.ds(pl.multiple_of(i * 64 + 8, 8), 64)
                if g == "c":
                    gated[o, 0:256] = rnd(rnd(acc_b[r, 384:640]) * rnd(acc_a[r, 128:384]))
                    gated[o, 256:384] = rnd(rnd(acc_a[r, 0:128]) * rnd(acc_a[r, 384:512]))
                else:
                    gated[o, :] = rnd(rnd(acc_da[r, 0:128]) * rnd(acc_da[r, 128:256]))
                return 0

            lax.fori_loop(0, TOK // 64, gate, 0)
            go(halo_copy(g))
            tp = taps[...].astype(F32)[:, lanes]

            def rows(i, first):
                block = gated[pl.ds(pl.multiple_of(i * ROWS, 32), ROWS + 8), :]
                if first:
                    keep = jnp.where(sp == 0, 0.0, 1.0)
                    rim = lax.broadcasted_iota(jnp.int32, (ROWS + 8, 1), 0) < 8
                    block = jnp.where(rim, block * keep, block)
                one = pltpu.roll(block, 1, 0)[8:, :]
                two = pltpu.roll(block, 2, 0)[8:, :]
                s = tp[0:1, :] * two + tp[1:2, :] * one + tp[2:3, :] * block[8:, :]
                r = pl.ds(pl.multiple_of(i * ROWS, 32), ROWS)
                if g == "c":
                    mix[self.place(i), 512:MIX] = (s * rnd(acc_b[r, 0:384])).astype(BF16)
                else:
                    late_mix[r, :] = (s * rnd(acc_db[r, :])).astype(BF16)

            def step(i, _):
                rows(i, False)
                return 0

            lax.fori_loop(1, 8, step, 0)
            halo_copy(g).wait_recv()
            rows(0, True)

        def load_out(self):
            for c in started_q:
                c.wait_send()
            for i in range(CHUNKS):
                for c in out_loads(i):
                    c.start()

        def pair_products(self, i):
            for c in out_loads(i):
                c.wait()
            w = out_block(i)
            if i >= 2:
                sib_copy(i - 2).wait_send()
            sib_send[i % 2] = mm(mix[0 : 4 * ROWS, :], w[...]).astype(BF16)
            sib_copy(i).start()
            own[i % 4] = mm(mix[4 * ROWS : TOK, :], w[...])

        def pair(self, c, d, r0, rows):
            at = slice(d * ROWS + r0, d * ROWS + r0 + rows)
            return own[c % 4, at, :] + sib_recv[c, at, :].astype(F32)

        def far(self, c):
            sib_copy(c).wait_recv()
            for side in (0, 1):
                far_send[c, side] = self.pair(c, 2, side * 48, 48).astype(BF16)
                go(far_copy(c, side))

        def near(self, c):
            far_copy(c, 0).wait_recv()
            near_send[c, 0, 0:48, :] = (self.pair(c, 1, 0, 48) + far_recv[c, 0].astype(F32)).astype(BF16)
            near_send[c, 0, 48:96, :] = self.pair(c, 1, 48, 48).astype(BF16)
            go(near_copy(c, 0))
            far_copy(c, 1).wait_recv()
            near_send[c, 1, 0:48, :] = self.pair(c, 3, 0, 48).astype(BF16)
            near_send[c, 1, 48:96, :] = (self.pair(c, 3, 48, 48) + far_recv[c, 1].astype(F32)).astype(BF16)
            go(near_copy(c, 1))

        def gather(self, c):
            near_copy(c, 0).wait_recv()
            near_copy(c, 1).wait_recv()
            total = self.pair(c, 0, 0, ROWS) + near_recv[c, 0].astype(F32) + near_recv[c, 1].astype(F32)
            inside[c * ROWS : (c + 1) * ROWS, :] = total

        def exchange(self):
            for d in (1, 7, 2, 6, 3, 5, 4):
                go(late_copy(d, True))
            late_recv[t] = late_mix[pl.ds(own_rows, ROWS), :]

        def last(self):
            for d in range(1, 8):
                late_copy(d, False).wait_recv()
            lhs = jnp.concatenate([late_recv[g] for g in range(8)], axis=1)
            for i in range(CHUNKS):
                k = slice(i * CW, (i + 1) * CW)
                out[:, k] = (inside[i * ROWS : (i + 1) * ROWS, :] + mm(lhs, wf[:, k])).astype(BF16)
            for i in range(CHUNKS - 2, CHUNKS):
                sib_copy(i).wait_send()
            for c in started:
                c.wait_send()

    plan(Device())


def layer(*args):
    any_ = pl.BlockSpec(memory_space=pl.ANY)
    vmem = pl.BlockSpec(memory_space=pltpu.VMEM)
    dma = pltpu.SemaphoreType.DMA

    def f32(*shape):
        return pltpu.VMEM(shape, F32)

    def bf16(*shape):
        return pltpu.VMEM(shape, BF16)

    return pl.pallas_call(
        layer_kernel,
        out_shape=jax.ShapeDtypeStruct((ROWS, MODEL), BF16),
        in_specs=[any_, vmem] + [any_] * 6 + [vmem] * 6 + [any_] * 2,
        out_specs=vmem,
        scratch_shapes=[
            bf16(TOK, MODEL),
            bf16(MODEL, 512),
            bf16(MODEL, 512),
            bf16(MODEL, 512),
            bf16(MODEL, 640),
            bf16(MODEL, 256),
            bf16(MODEL, 128),
            bf16(8 * LATE, MODEL),
            f32(TOK, 512),
            f32(TOK, 640),
            f32(TOK, 256),
            f32(TOK, 128),
            bf16(TOK, 2 * KEY),
            bf16(TOK, 2 * KEY),
            bf16(TOK, 2 * VAL),
            f32(TOK, 2 * KEY),
            f32(TOK, 2 * KEY),
            f32(8, TOK),
            f32(TOK, 2 * VAL),
            bf16(TOK, 2 * KEY),
            f32(2 * VAL, KEY),
            f32(8, 2 * KEY),
            bf16(2, 2 * VAL, KEY),
            f32(2, 8, 2 * KEY),
            bf16(6, 2 * VAL, KEY),
            f32(6, 8, 2 * KEY),
            f32(TOK + 8, EARLY),
            f32(TOK + 8, LATE),
            bf16(TOK, MIX),
            bf16(TOK, LATE),
            bf16(8, ROWS, LATE),
            f32(4, 4 * ROWS, CW),
            bf16(2, 4 * ROWS, CW),
            bf16(CHUNKS, 4 * ROWS, CW),
            bf16(CHUNKS, 2, 48, CW),
            bf16(CHUNKS, 2, 48, CW),
            bf16(CHUNKS, 2, ROWS, CW),
            bf16(CHUNKS, 2, ROWS, CW),
            dma((12,)),
            dma((2 * CHUNKS,)),
            dma((6, 20)),
            dma((6, 20)),
            dma((20,)),
            dma((20,)),
            dma((16,)),
            dma((16,)),
            dma((2,)),
            dma((2,)),
            dma((7,)),
            dma((7,)),
            dma((CHUNKS,)),
            dma((CHUNKS,)),
            dma((CHUNKS, 2)),
            dma((CHUNKS, 2)),
            dma((CHUNKS, 2)),
            dma((CHUNKS, 2)),
        ],
        compiler_params=pltpu.CompilerParams(
            collective_id=0, has_side_effects=True, vmem_limit_bytes=67_000_000
        ),
        name="layer",
    )(*args)


def body(
    hidden_activations,
    entry_rescale_vector,
    probe_matrix,
    lookup_address_matrix,
    payload_matrix,
    postfilter_switch_matrix,
    prefilter_switch_matrix,
    filter_source_matrix,
    forget_left_factor,
    forget_right_factor,
    forget_offset_per_feature,
    forget_spike_additions,
    subspace_rescale_vector,
    depthwise_filter_taps,
    mixer_result_matrix,
    filter_result_matrix,
):
    return layer(
        hidden_activations,
        entry_rescale_vector.reshape(32, 128),
        probe_matrix,
        lookup_address_matrix,
        payload_matrix,
        postfilter_switch_matrix,
        prefilter_switch_matrix,
        filter_source_matrix,
        forget_left_factor.T,
        forget_right_factor,
        forget_offset_per_feature[None, :],
        forget_spike_additions,
        subspace_rescale_vector,
        depthwise_filter_taps,
        mixer_result_matrix,
        filter_result_matrix,
    )


def solution(mesh):
    split = Mesh(mesh.devices.reshape(4, 4, mesh.shape["tp"]), ("sp_0", "sp_1", "tp"))
    in_specs = (
        P(SP_TP, None),
        P(),
        P(SP, "tp"),
        P(SP, "tp"),
        P(SP, "tp"),
        P(SP, "tp"),
        P(SP, "tp"),
        P(SP, "tp"),
        P(),
        P(None, "tp"),
        P("tp"),
        P("tp", SP),
        P("tp", None),
        P(None, "tp"),
        P("tp", None),
        P("tp", None),
    )
    out_specs = P(SP_TP, None)
    return jax.shard_map(body, mesh=split, in_specs=in_specs, out_specs=out_specs, check_vma=False)
```

```python
import jax
import jax.numpy as jnp
from jax import lax
from jax.experimental import pallas as pl
from jax.experimental.pallas import tpu as pltpu
from jax.sharding import Mesh
from jax.sharding import PartitionSpec as P

MESH = pl.DeviceIdType.MESH
SP = ("sp_0", "sp_1")
SP_TP = ("sp_0", "sp_1", "tp")
F32 = jnp.float32
BF16 = jnp.bfloat16
HIGHEST = lax.Precision.HIGHEST

BLOCK = 64
ROWS = 96
TOK = 768
MODEL = 4096
KB = 256
LATE = 256
EARLY = 512 - LATE
MIX = 512 + EARLY
CHUNKS = 8
CW = MODEL // CHUNKS
KEY, VAL = 128, 256
EPS = 1e-06
DELTA = (0, 3, 1, 2)


def nt(a, b):
    return lax.dot_general(a, b, (((1,), (1,)), ((), ())), preferred_element_type=F32)


def tn(a, b):
    return lax.dot_general(a, b, (((0,), (0,)), ((), ())), preferred_element_type=F32)


def mm(a, b):
    return jnp.dot(a, b, preferred_element_type=F32)


SEND, WAIT, RUN = "send", "wait", "run"
W, R, S = "w", "r", "s"
Q, E, C, D = "q", "e", "c", "d"
X, F, H = "x", "f", "h"
T_NORM = "norm"
T_LOW_RANK = "low_rank"
T_RATE = "rate"
T_SUFFIX = "suffix"
T_PROJECT = "project"
T_KEY_STATE = "key_state"
T_ATTEND = "attend"
T_FOLD_Y = "fold_y"
T_FOLD_Z = "fold_z"
T_GATE = "gate"
T_CONV = "conv"
T_FIRST_ROWS = "first_rows"
T_EXCHANGE = "exchange"
T_LOAD_H = "load_h"
T_START_H = "start_h"
T_PAIR_PRODUCTS = "pair_products"
T_FAR = "far"
T_NEAR = "near"
T_GATHER = "gather"
T_COLLECT = "collect"
T_LAST = "last"
ORDER = (
    (SEND, W, Q, 0, 0), (SEND, W, Q, 1, 4), (SEND, W, Q, 0, 1), (SEND, W, Q, 1, 5), (SEND, W, Q, 1, 0),
    (SEND, W, Q, 0, 4), (SEND, W, Q, 1, 1), (SEND, W, Q, 0, 5), (RUN, T_NORM), (SEND, R, X, 0), (SEND, R, X, 2),
    (SEND, R, X, 6), (SEND, W, E, 0, 0), (SEND, W, E, 0, 1), (SEND, W, E, 1, 0), (SEND, W, E, 1, 1),
    (SEND, W, E, 0, 4), (SEND, W, E, 0, 5), (SEND, W, E, 1, 4), (SEND, W, E, 1, 5), (SEND, R, X, 1),
    (SEND, R, X, 3), (WAIT, W, Q, 1, 0), (SEND, W, Q, 1, 6), (SEND, W, Q, 1, 7), (WAIT, W, Q, 0, 0),
    (SEND, W, Q, 0, 6), (SEND, W, Q, 0, 7), (SEND, W, Q, 0, 2), (WAIT, W, Q, 0, 1), (SEND, W, Q, 0, 3),
    (SEND, W, Q, 1, 2), (WAIT, W, Q, 1, 1), (SEND, W, Q, 1, 3), (SEND, W, Q, 0, 8), (SEND, W, Q, 0, 9),
    (SEND, W, Q, 1, 8), (SEND, W, Q, 1, 9), (WAIT, R, X, 0), (SEND, R, X, 4), (WAIT, R, X, 2), (SEND, R, X, 5),
    (WAIT, W, Q, 0, 4), (SEND, W, Q, 0, 12), (WAIT, W, Q, 0, 5), (SEND, W, Q, 0, 13), (WAIT, W, Q, 1, 4),
    (SEND, W, Q, 1, 12), (WAIT, W, Q, 1, 5), (SEND, W, Q, 1, 13), (WAIT, W, Q, 0, 2), (WAIT, W, Q, 0, 3),
    (SEND, W, Q, 0, 10), (SEND, W, Q, 0, 11), (WAIT, W, Q, 1, 2), (WAIT, W, Q, 1, 3), (SEND, W, Q, 1, 10),
    (SEND, W, Q, 1, 11), (WAIT, R, X, 1), (SEND, R, X, 7), (WAIT, R, X, 3), (SEND, R, X, 8), (WAIT, W, Q, 0, 6),
    (SEND, W, Q, 0, 14), (WAIT, W, Q, 0, 7), (SEND, W, Q, 0, 15), (WAIT, W, Q, 1, 6), (SEND, W, Q, 1, 14),
    (WAIT, W, Q, 1, 7), (SEND, W, Q, 1, 15), (WAIT, W, E, 1, 0), (SEND, W, E, 1, 2), (WAIT, W, E, 1, 1),
    (SEND, W, E, 1, 3), (WAIT, W, E, 0, 0), (SEND, W, E, 0, 2), (WAIT, W, E, 0, 1), (SEND, W, E, 0, 3),
    (WAIT, W, Q, 0, 8), (SEND, W, Q, 0, 16), (WAIT, W, Q, 0, 9), (SEND, W, Q, 0, 17), (WAIT, W, Q, 1, 8),
    (SEND, W, Q, 1, 16), (WAIT, W, Q, 1, 9), (SEND, W, Q, 1, 17), (SEND, W, E, 0, 6), (SEND, W, E, 0, 7),
    (SEND, W, E, 1, 6), (SEND, W, E, 1, 7), (WAIT, R, X, 4), (WAIT, R, X, 5), (SEND, R, X, 9), (SEND, R, F, 6),
    (SEND, R, F, 0), (SEND, R, F, 2), (WAIT, W, Q, 0, 10), (SEND, W, Q, 0, 18), (WAIT, W, Q, 0, 11),
    (SEND, W, Q, 0, 19), (WAIT, W, Q, 1, 10), (SEND, W, Q, 1, 18), (WAIT, W, Q, 1, 11), (SEND, W, Q, 1, 19),
    (WAIT, W, E, 0, 4), (SEND, W, E, 0, 12), (WAIT, W, E, 0, 5), (SEND, W, E, 0, 13), (WAIT, W, E, 1, 4),
    (SEND, W, E, 1, 12), (WAIT, W, E, 1, 5), (SEND, W, E, 1, 13), (WAIT, W, Q, 0, 12), (WAIT, W, Q, 0, 13),
    (WAIT, R, X, 6), (WAIT, R, X, 7), (WAIT, R, X, 8), (WAIT, R, X, 9), (RUN, T_PROJECT, Q, 0, 0),
    (WAIT, W, E, 0, 2), (WAIT, W, E, 0, 3), (SEND, W, E, 0, 10), (SEND, W, E, 0, 11), (WAIT, W, E, 1, 2),
    (WAIT, W, E, 1, 3), (SEND, W, E, 1, 10), (SEND, W, E, 1, 11), (WAIT, W, Q, 0, 14), (WAIT, W, Q, 0, 15),
    (RUN, T_PROJECT, Q, 0, 1), (SEND, W, E, 0, 8), (SEND, W, E, 0, 9), (SEND, W, E, 1, 8), (SEND, W, E, 1, 9),
    (WAIT, W, Q, 1, 12), (WAIT, W, Q, 1, 13), (RUN, T_PROJECT, Q, 1, 0), (WAIT, W, Q, 0, 16),
    (WAIT, W, Q, 0, 17), (RUN, T_PROJECT, Q, 0, 2), (SEND, W, C, 0, 0), (SEND, W, C, 0, 1), (SEND, W, C, 1, 0),
    (SEND, W, C, 1, 1), (WAIT, W, Q, 1, 14), (WAIT, W, Q, 1, 15), (RUN, T_PROJECT, Q, 1, 1), (SEND, R, F, 1),
    (SEND, R, F, 3), (WAIT, W, Q, 1, 16), (WAIT, W, Q, 1, 17), (RUN, T_PROJECT, Q, 1, 2), (RUN, T_LOW_RANK),
    (WAIT, W, E, 0, 6), (SEND, W, E, 0, 14), (SEND, W, C, 0, 4), (WAIT, W, E, 0, 7), (SEND, W, E, 0, 15),
    (SEND, W, C, 0, 5), (WAIT, W, E, 1, 6), (SEND, W, E, 1, 14), (SEND, W, C, 1, 4), (WAIT, W, E, 1, 7),
    (SEND, W, E, 1, 15), (SEND, W, C, 1, 5), (RUN, T_RATE, 0, 2), (RUN, T_RATE, 2, 4), (RUN, T_RATE, 4, 6),
    (RUN, T_SUFFIX), (WAIT, W, E, 0, 10), (SEND, W, E, 0, 18), (WAIT, W, E, 0, 11), (SEND, W, E, 0, 19),
    (WAIT, W, E, 1, 10), (SEND, W, E, 1, 18), (WAIT, W, E, 1, 11), (SEND, W, E, 1, 19), (WAIT, W, Q, 0, 18),
    (WAIT, W, Q, 0, 19), (RUN, T_PROJECT, Q, 0, 3), (WAIT, W, E, 0, 8), (SEND, W, E, 0, 16), (WAIT, W, E, 0, 9),
    (SEND, W, E, 0, 17), (WAIT, W, E, 1, 8), (SEND, W, E, 1, 16), (WAIT, W, E, 1, 9), (SEND, W, E, 1, 17),
    (WAIT, W, Q, 1, 18), (WAIT, W, Q, 1, 19), (RUN, T_PROJECT, Q, 1, 3), (WAIT, W, C, 0, 0), (SEND, W, C, 0, 2),
    (WAIT, W, C, 0, 1), (SEND, W, C, 0, 3), (WAIT, W, C, 1, 0), (SEND, W, C, 1, 2), (WAIT, W, C, 1, 1),
    (SEND, W, C, 1, 3), (RUN, T_KEY_STATE), (WAIT, W, E, 0, 12), (WAIT, W, E, 0, 13), (RUN, T_PROJECT, E, 0, 0),
    (SEND, S, 0, 0), (SEND, S, 0, 1), (SEND, W, C, 1, 6), (SEND, W, C, 1, 7), (WAIT, R, F, 0), (SEND, R, F, 4),
    (WAIT, R, F, 2), (SEND, R, F, 5), (WAIT, W, E, 0, 14), (WAIT, W, E, 0, 15), (RUN, T_PROJECT, E, 0, 1),
    (WAIT, W, E, 1, 12), (WAIT, W, E, 1, 13), (RUN, T_PROJECT, E, 1, 0), (WAIT, W, E, 1, 14),
    (WAIT, W, E, 1, 15), (RUN, T_PROJECT, E, 1, 1), (SEND, W, C, 0, 6), (SEND, W, C, 0, 7), (SEND, W, C, 1, 8),
    (SEND, W, C, 1, 9), (WAIT, W, E, 0, 16), (WAIT, W, E, 0, 17), (RUN, T_PROJECT, E, 0, 2),
    (WAIT, W, E, 0, 18), (WAIT, W, E, 0, 19), (RUN, T_PROJECT, E, 0, 3), (WAIT, W, E, 1, 16),
    (WAIT, W, E, 1, 17), (RUN, T_PROJECT, E, 1, 2), (WAIT, W, E, 1, 18), (WAIT, W, E, 1, 19),
    (RUN, T_PROJECT, E, 1, 3), (WAIT, R, F, 1), (SEND, R, F, 7), (WAIT, R, F, 3), (SEND, R, F, 8),
    (RUN, T_LOAD_H), (SEND, W, C, 0, 8), (SEND, W, C, 0, 9), (RUN, T_ATTEND, 0, 3), (RUN, T_ATTEND, 3, 6),
    (WAIT, W, C, 1, 2), (WAIT, W, C, 1, 3), (SEND, W, C, 1, 10), (SEND, W, C, 1, 11), (RUN, T_ATTEND, 6, 9),
    (RUN, T_START_H), (SEND, R, H, 6), (RUN, T_ATTEND, 9, 12), (SEND, R, H, 0), (SEND, R, H, 2),
    (WAIT, S, 0, 0), (SEND, S, 0, 2), (WAIT, S, 0, 1), (SEND, S, 0, 3), (WAIT, W, C, 0, 2), (WAIT, W, C, 0, 3),
    (SEND, W, C, 0, 10), (SEND, W, C, 0, 11), (WAIT, W, C, 1, 4), (SEND, W, C, 1, 12), (WAIT, W, C, 1, 5),
    (SEND, W, C, 1, 13), (WAIT, W, C, 1, 8), (SEND, W, C, 1, 16), (WAIT, W, C, 1, 9), (SEND, W, C, 1, 17),
    (WAIT, R, F, 4), (WAIT, R, F, 5), (SEND, R, F, 9), (WAIT, W, C, 0, 4), (SEND, W, C, 0, 12),
    (WAIT, W, C, 0, 5), (SEND, W, C, 0, 13), (WAIT, W, C, 1, 6), (SEND, W, C, 1, 14), (WAIT, W, C, 1, 7),
    (SEND, W, C, 1, 15), (WAIT, S, 0, 2), (WAIT, S, 0, 3), (RUN, T_FOLD_Y), (WAIT, W, C, 0, 8),
    (SEND, W, C, 0, 16), (WAIT, W, C, 0, 9), (SEND, W, C, 0, 17), (SEND, S, 1, 0), (SEND, S, 1, 1),
    (WAIT, W, C, 0, 6), (SEND, W, C, 0, 14), (WAIT, W, C, 0, 7), (SEND, W, C, 0, 15), (WAIT, W, C, 1, 12),
    (WAIT, W, C, 1, 13), (RUN, T_PROJECT, C, 1, 0), (WAIT, W, C, 1, 10), (SEND, W, C, 1, 18),
    (WAIT, W, C, 1, 11), (SEND, W, C, 1, 19), (SEND, R, H, 1), (SEND, R, H, 3), (WAIT, W, C, 0, 10),
    (SEND, W, C, 0, 18), (WAIT, W, C, 0, 11), (SEND, W, C, 0, 19), (SEND, W, D, 0, 0), (SEND, W, D, 0, 1),
    (SEND, W, D, 1, 0), (SEND, W, D, 1, 1), (WAIT, W, C, 1, 14), (WAIT, W, C, 1, 15), (RUN, T_PROJECT, C, 1, 1),
    (WAIT, W, C, 0, 12), (WAIT, W, C, 0, 13), (RUN, T_PROJECT, C, 0, 0), (WAIT, W, C, 1, 16),
    (WAIT, W, C, 1, 17), (RUN, T_PROJECT, C, 1, 2), (WAIT, S, 1, 0), (SEND, S, 1, 2), (WAIT, S, 1, 1),
    (SEND, S, 1, 3), (SEND, W, D, 0, 4), (SEND, W, D, 0, 5), (SEND, W, D, 1, 4), (SEND, W, D, 1, 5),
    (WAIT, W, C, 0, 14), (WAIT, W, C, 0, 15), (RUN, T_PROJECT, C, 0, 1), (WAIT, W, C, 0, 16),
    (WAIT, W, C, 0, 17), (RUN, T_PROJECT, C, 0, 2), (WAIT, W, C, 1, 18), (WAIT, W, C, 1, 19),
    (RUN, T_PROJECT, C, 1, 3), (WAIT, W, C, 0, 18), (WAIT, W, C, 0, 19), (RUN, T_PROJECT, C, 0, 3),
    (RUN, T_GATE, C), (WAIT, R, H, 0), (SEND, R, H, 4), (WAIT, R, H, 2), (SEND, R, H, 5), (RUN, T_CONV, C),
    (WAIT, W, D, 0, 0), (SEND, W, D, 0, 2), (WAIT, W, D, 0, 1), (SEND, W, D, 0, 3), (SEND, W, D, 0, 6),
    (SEND, W, D, 0, 7), (WAIT, W, D, 1, 0), (SEND, W, D, 1, 6), (SEND, W, D, 1, 7), (WAIT, S, 1, 2),
    (WAIT, S, 1, 3), (RUN, T_FOLD_Z), (RUN, T_FIRST_ROWS, C), (RUN, T_PAIR_PRODUCTS, 0),
    (RUN, T_PAIR_PRODUCTS, 1), (SEND, W, D, 1, 2), (WAIT, W, D, 1, 1), (SEND, W, D, 1, 3),
    (RUN, T_PAIR_PRODUCTS, 2), (RUN, T_PAIR_PRODUCTS, 3), (WAIT, R, H, 1), (SEND, R, H, 7), (WAIT, R, H, 3),
    (SEND, R, H, 8), (RUN, T_FAR, 0), (RUN, T_FAR, 1), (WAIT, W, D, 0, 4), (SEND, W, D, 0, 12),
    (WAIT, W, D, 0, 5), (SEND, W, D, 0, 13), (WAIT, W, D, 1, 4), (SEND, W, D, 1, 12), (WAIT, W, D, 1, 5),
    (SEND, W, D, 1, 13), (RUN, T_FAR, 2), (RUN, T_FAR, 3), (WAIT, W, D, 0, 2), (WAIT, W, D, 0, 3),
    (SEND, W, D, 0, 10), (SEND, W, D, 0, 11), (SEND, W, D, 1, 8), (SEND, W, D, 1, 9), (WAIT, W, D, 0, 6),
    (SEND, W, D, 0, 14), (WAIT, W, D, 0, 7), (SEND, W, D, 0, 15), (WAIT, W, D, 1, 2), (WAIT, W, D, 1, 3),
    (SEND, W, D, 1, 10), (SEND, W, D, 1, 11), (SEND, W, D, 0, 8), (SEND, W, D, 0, 9), (WAIT, W, D, 0, 12),
    (WAIT, W, D, 0, 13), (RUN, T_PROJECT, D, 0, 0), (WAIT, W, D, 1, 12), (WAIT, W, D, 1, 13),
    (RUN, T_PROJECT, D, 1, 0), (WAIT, R, H, 4), (WAIT, R, H, 5), (SEND, R, H, 9), (WAIT, W, D, 1, 6),
    (SEND, W, D, 1, 14), (WAIT, W, D, 1, 7), (SEND, W, D, 1, 15), (RUN, T_NEAR, 0), (WAIT, W, D, 0, 10),
    (SEND, W, D, 0, 18), (WAIT, W, D, 0, 11), (SEND, W, D, 0, 19), (WAIT, W, D, 1, 8), (SEND, W, D, 1, 16),
    (WAIT, W, D, 1, 9), (SEND, W, D, 1, 17), (RUN, T_NEAR, 1), (RUN, T_NEAR, 2), (WAIT, W, D, 0, 14),
    (WAIT, W, D, 0, 15), (RUN, T_PROJECT, D, 0, 1), (RUN, T_NEAR, 3), (WAIT, W, D, 1, 10), (SEND, W, D, 1, 18),
    (WAIT, W, D, 1, 11), (SEND, W, D, 1, 19), (RUN, T_GATHER, 0), (RUN, T_PAIR_PRODUCTS, 4), (WAIT, W, D, 0, 8),
    (SEND, W, D, 0, 16), (WAIT, W, D, 0, 9), (SEND, W, D, 0, 17), (WAIT, W, D, 1, 14), (WAIT, W, D, 1, 15),
    (RUN, T_PROJECT, D, 1, 1), (RUN, T_GATHER, 1), (RUN, T_PAIR_PRODUCTS, 5), (RUN, T_FAR, 4),
    (WAIT, W, D, 1, 16), (WAIT, W, D, 1, 17), (RUN, T_PROJECT, D, 1, 2), (RUN, T_GATHER, 2),
    (RUN, T_PAIR_PRODUCTS, 6), (RUN, T_FAR, 5), (WAIT, W, D, 1, 18), (WAIT, W, D, 1, 19),
    (RUN, T_PROJECT, D, 1, 3), (RUN, T_GATHER, 3), (RUN, T_PAIR_PRODUCTS, 7), (RUN, T_NEAR, 4),
    (WAIT, W, D, 0, 16), (WAIT, W, D, 0, 17), (RUN, T_PROJECT, D, 0, 2), (WAIT, W, D, 0, 18),
    (WAIT, W, D, 0, 19), (RUN, T_PROJECT, D, 0, 3), (RUN, T_NEAR, 5), (RUN, T_GATE, D), (RUN, T_CONV, D),
    (RUN, T_FAR, 6), (RUN, T_FAR, 7), (RUN, T_GATHER, 4), (RUN, T_FIRST_ROWS, D), (RUN, T_EXCHANGE),
    (RUN, T_GATHER, 5), (RUN, T_NEAR, 6), (RUN, T_NEAR, 7), (WAIT, R, F, 6), (WAIT, R, F, 7), (WAIT, R, F, 8),
    (WAIT, R, F, 9), (WAIT, R, H, 6), (WAIT, R, H, 7), (WAIT, R, H, 8), (WAIT, R, H, 9), (RUN, T_COLLECT),
    (RUN, T_LAST, 0), (RUN, T_LAST, 1), (RUN, T_LAST, 2), (RUN, T_LAST, 3), (RUN, T_LAST, 4),
    (RUN, T_GATHER, 6), (RUN, T_LAST, 5), (RUN, T_LAST, 6), (RUN, T_GATHER, 7), (RUN, T_LAST, 7),
)


def layer_kernel(
    x_in,
    gain,
    w_q,
    w_k,
    w_v,
    w_out,
    w_in,
    w_src,
    left,
    right,
    offset,
    spikes,
    head_gain,
    taps,
    w_a,
    w_c,
    out,
    xs,
    qab,
    ca,
    cb,
    da,
    db,
    wf,
    wo,
    acc_a,
    acc_b,
    krows,
    vrows,
    low,
    within,
    tail,
    spk,
    inside,
    q_far,
    state,
    prefix,
    st_send,
    dec_send,
    st_recv,
    dec_recv,
    gated_c,
    gated_d,
    mix,
    late_mix,
    late_recv,
    own,
    sib_send,
    sib_recv,
    far_send,
    far_recv,
    near_send,
    near_recv,
    load_sem,
    out_sem,
    w_send,
    w_recv,
    x_send,
    x_recv,
    s_send,
    s_recv,
    h_send,
    h_recv,
    e_send,
    e_recv,
    ss,
    sr,
    fs,
    fr,
    ns,
    nr,
    free_sem,
):
    z = lax.axis_index("sp_0")
    y = lax.axis_index("sp_1")
    t = lax.axis_index("tp")
    core = t % 2
    xi = t // 2
    sp = z * 4 + y
    sp_next = (sp + 1) % 16
    sp_prev = (sp + 15) % 16
    to_next = {"sp_0": sp_next // 4, "sp_1": sp_next % 4}
    to_prev = {"sp_0": sp_prev // 4, "sp_1": sp_prev % 4}
    to_sib = {"tp": xi * 2 + (1 - core)}

    def at_z(d):
        return {"sp_0": (z + d) % 4}

    def at_y(d):
        return {"sp_1": (y + d) % 4}

    def at_x(d):
        return {"tp": ((xi + d) % 4) * 2 + core}

    def remote(ref, dst, sems, at, to):
        return pltpu.make_async_remote_copy(
            src_ref=ref,
            dst_ref=dst,
            send_sem=sems[0].at[at],
            recv_sem=sems[1].at[at],
            device_id=to,
            device_id_type=MESH,
        )

    own0 = pl.ds(pl.multiple_of(sp * KB, KB), KB)
    own1 = pl.ds(pl.multiple_of((y * 4 + z) * KB, KB), KB)
    own1_v = pl.ds(pl.multiple_of(MODEL + (y * 4 + z) * KB, KB), KB)
    own_rows = pl.multiple_of(t * ROWS, 32)
    loads = [
        (x_in, xs.at[pl.ds(own_rows, ROWS), :]),
        (w_k, qab.at[own0, 0:256]),
        (w_v.at[:, 0:128], qab.at[own0, 256:384]),
        (w_q.at[:, 0:128], qab.at[own0, 384:512]),
        (w_v.at[:, 128:512], qab.at[own1_v, 0:384]),
        (w_q.at[:, 128:256], qab.at[own1_v, 384:512]),
        (w_in.at[:, 128:256], ca.at[own0, 0:128]),
        (w_src.at[:, 0:256], ca.at[own0, 128:384]),
        (w_out.at[:, 0:256], cb.at[own1, 0:256]),
        (w_in.at[:, 0:128], cb.at[own1, 256:384]),
        (w_in.at[:, 384:512], da.at[own0, 0:128]),
        (w_src.at[:, 256:512], da.at[own0, 128:384]),
        (w_out.at[:, 256:512], db.at[own1, 0:256]),
        (w_in.at[:, 256:384], db.at[own1, 256:384]),
        (w_c.at[EARLY : EARLY + 128, :], wf.at[pl.ds(pl.multiple_of(t * 128, 128), 128), :]),
    ]
    loads = [pltpu.make_async_copy(a, b, load_sem.at[i]) for i, (a, b) in enumerate(loads)]
    for c in loads:
        c.start()

    barrier = pltpu.get_barrier_semaphore()
    peers = [at_z(1), at_z(3), at_y(1), at_y(3), to_next, to_prev] + [{"tp": (t + d) % 8} for d in range(1, 8)]
    for p in peers:
        pl.semaphore_signal(barrier, inc=1, device_id=p, device_id_type=MESH)

    def h_loads():
        return [
            pltpu.make_async_copy(
                w_c.at[EARLY + 128 : 512, pl.ds(i * 512, 512)],
                qab.at[pl.ds(pl.multiple_of(t * 1024 + i * 128, 128), 128), :],
                load_sem.at[14 + i],
            )
            for i in range(8)
        ]

    def out_loads(i):
        cols = pl.ds(i * CW, CW)
        return (
            pltpu.make_async_copy(w_a.at[:, cols], wo.at[i % 3, 0:512, :], out_sem.at[2 * i]),
            pltpu.make_async_copy(w_c.at[0:EARLY, cols], wo.at[i % 3, 512:MIX, :], out_sem.at[2 * i + 1]),
        )

    for c in loads[1:]:
        c.wait()
    pl.semaphore_wait(barrier, len(peers))

    started = []
    started_q = []

    def go(c, group=None):
        c.start()
        (started_q if group in ("q", "e") else started).append(c)

    bufs = {"q": (qab, qab), "e": (qab, qab), "c": (ca, cb), "d": (da, db)}
    first_row = {"q": (0, MODEL), "e": (0, MODEL), "c": (0, 0), "d": (0, 0)}
    lanes = {"q": slice(0, 384), "e": slice(384, 512), "c": slice(0, 384), "d": slice(0, 384)}
    base = {"q": 0, "c": 2, "d": 4, "e": 6}
    rings = {"x": (xs, ROWS, 0), "f": (wf, 128, 10), "h": (qab, 1024, 20)}
    xm, xp, xf = (xi + 3) % 4, (xi + 1) % 4, (xi + 2) % 4

    def w_copy(g, path, slot, du, dv, axis, step, row=0, rows=KB):
        u0, v0 = (z, y) if path == 0 else (y, z)
        j = ((u0 + du) % 4) * 4 + (v0 + dv) % 4
        ref = bufs[g][path].at[pl.ds(pl.multiple_of(first_row[g][path] + j * KB + row, 128), rows), lanes[g]]
        to = at_z(step) if (axis == 0) == (path == 0) else at_y(step)
        return remote(ref, ref, (w_send, w_recv), (base[g] + path, slot), to)

    def ring_copy(n, slot, x_from, top, halves, to, c=None):
        buf, rows, first = rings[n]
        half = rows // 2
        at = (x_from * 2 + (core if c is None else c)) * rows + (0 if top else half)
        ref = buf.at[pl.ds(pl.multiple_of(at, 16), half * halves), :]
        return remote(ref, ref, (x_send, x_recv), first + slot, to)

    right_x, left_x = at_x(1), at_x(3)

    def st_copy(ph, slot):
        to = (at_y if ph == 0 else at_z)(1 if slot % 2 == 0 else 3)
        i = ph * 3
        if slot < 2:
            a, b = st_send.at[ph], st_recv.at[i + 2 * slot]
        else:
            half = pl.ds((slot - 2) * VAL, VAL)
            a, b = st_recv.at[i + 2 * (slot - 2), half, :], st_recv.at[i + 1, half, :]
        return remote(a, b, (s_send, s_recv), ph * 8 + slot, to)

    def dec_copy(ph, slot):
        to = (at_y if ph == 0 else at_z)(1 if slot != 1 else 3)
        i = ph * 3
        if slot < 2:
            a, b = dec_send.at[ph], dec_recv.at[i + 2 * slot]
        else:
            a, b = dec_recv.at[i], dec_recv.at[i + 1]
        return remote(a, b, (s_send, s_recv), ph * 8 + 4 + slot, to)

    def halo_copy(g):
        buf = gated_c if g == "c" else gated_d
        i = 0 if g == "c" else 1
        return remote(buf.at[pl.ds(TOK, 8), :], buf.at[pl.ds(0, 8), :], (h_send, h_recv), i, to_next)

    def sib_copy(c):
        return remote(sib_send.at[c % 2], sib_recv.at[c], (ss, sr), c, to_sib)

    def far_copy(c, side):
        return remote(far_send.at[c % 4, side], far_recv.at[c, side], (fs, fr), (c, side), right_x if side == 0 else left_x)

    def near_copy(c, side):
        return remote(near_send.at[c % 4, side], near_recv.at[c, side], (ns, nr), (c, side), right_x if side == 0 else left_x)

    def late_copy(d, sending):
        g = (t + d) % 8
        me = t if sending else (t + 8 - d) % 8
        src = late_mix.at[pl.ds(pl.multiple_of(g * ROWS, 32), ROWS), :]
        return remote(src, late_recv.at[me], (e_send, e_recv), d - 1, {"tp": g})

    def w_sent(g, p, slot):
        if slot < 2:
            return w_copy(g, p, slot, 0, 0, 0, 1 + 2 * slot)
        if slot < 4:
            return w_copy(g, p, slot, 3 if slot == 2 else 1, 0, 0, 1 if slot == 2 else 3, 128 * (slot - 2), 128)
        k, side = DELTA[(slot - 4) % 8 // 2], slot % 2
        if slot < 12:
            return w_copy(g, p, slot, k, 0, 1, 1 + 2 * side)
        return w_copy(g, p, slot, k, 1 if side else 3, 1, 1 + 2 * side, 128 * side, 128)

    def w_came(g, p, slot):
        side = slot % 2
        step, row = 1 + 2 * side, 128 * side
        if slot < 2:
            return w_copy(g, p, slot, 1 if side else 3, 0, 0, step)
        if slot < 4:
            return w_copy(g, p, slot, 2, 0, 0, step, row, 128)
        k = DELTA[(slot - 4) % 8 // 2]
        if slot < 12:
            return w_copy(g, p, slot, k, 1 if side else 3, 1, step)
        return w_copy(g, p, slot, k, 2, 1, step, row, 128)

    ring_sent = (
        (0, True, 1, 1), (0, False, 1, 1), (0, False, 1, 3), (0, True, 1, 3), (3, True, 1, 1), (1, False, 1, 3),
        (0, True, 2, 0), (3, True, 2, 0), (1, True, 2, 0), (2, True, 2, 0),
    )
    ring_came = (
        (3, True, 1, 1), (3, False, 1, 1), (1, False, 1, 3), (1, True, 1, 3), (2, True, 1, 1), (2, False, 1, 3),
        (0, True, 2, 0), (3, True, 2, 0), (1, True, 2, 0), (2, True, 2, 0),
    )

    def ring(n, slot, came):
        d, top, halves, step = (ring_came if came else ring_sent)[slot]
        to = to_sib if step == 0 else at_x(step)
        other = came and step == 0
        return ring_copy(n, slot, (xi + d) % 4, top, halves, to, 1 - core if other else None)

    def head(h):
        return slice(h * KEY, (h + 1) * KEY), slice(h * VAL, (h + 1) * VAL)

    class Device:
        def send(self, kind, *a):
            if kind == "w":
                go(w_sent(*a), a[0])
            elif kind == "r":
                go(ring(*a, False))
            else:
                go(st_copy(*a))
                if a[1] < 3:
                    go(dec_copy(*a))

        def wait(self, kind, *a):
            if kind == "w":
                w_came(*a).wait_recv()
            elif kind == "r":
                ring(*a, True).wait_recv()
            elif kind == "s":
                st_copy(*a).wait_recv()
                if a[1] < 3:
                    dec_copy(*a).wait_recv()

        def norm(self):
            loads[0].wait()

            def step(i, _):
                r = pl.ds(pl.multiple_of(own_rows + i * 16, 16), 16)
                v = xs[r, :].astype(F32)
                inv = lax.rsqrt(jnp.mean(v * v, axis=-1, keepdims=True) + EPS)
                g = gain[...].astype(F32)
                for c in range(32):
                    k = slice(c * 128, (c + 1) * 128)
                    xs[r, k] = (v[:, k] * inv * g[c : c + 1, :]).astype(BF16)
                return 0

            lax.fori_loop(0, ROWS // 16, step, 0)
            spk[...] = jnp.zeros_like(spk)
            spk[0:2, :] = spikes[...]
            for i in range(3):
                for c in out_loads(i):
                    c.start()

        def low_rank(self):
            low[...] = nt(xs[...], left[...]).astype(BF16)

        def rate(self, lo, hi):
            lane_head = lax.broadcasted_iota(jnp.int32, (8, 2 * KEY), 1) // KEY
            pick = jnp.where(lax.broadcasted_iota(jnp.int32, (8, 2 * KEY), 0) == lane_head, 1.0, 0.0).astype(F32)
            row = lax.broadcasted_iota(jnp.int32, (128, 128), 0)
            col = lax.broadcasted_iota(jnp.int32, (128, 128), 1)
            low_tri = jnp.where((row >= col) & (row // BLOCK == col // BLOCK), 1.0, 0.0).astype(F32)

            def step(i, _):
                r = pl.ds(pl.multiple_of(i * 128, 128), 128)
                g = mm(low[r, :], right[...]) + offset[...]
                ls = jnp.minimum(g, 0.0) - jnp.log1p(jnp.exp(-jnp.abs(g)))
                spike = lax.dot_general(
                    spk[:, r], pick, (((0,), (0,)), ((), ())), precision=HIGHEST, preferred_element_type=F32
                )
                within[r, :] = jnp.dot(
                    low_tri, ls * (1.0 / 16.0) + spike, precision=HIGHEST, preferred_element_type=F32
                )
                return 0

            lax.fori_loop(lo, hi, step, 0)

        def suffix(self):
            prefix[0:1, :] = jnp.zeros((1, 2 * KEY), F32)

            def back(i, _):
                n = TOK // BLOCK - 1 - i
                w = within[pl.ds(pl.multiple_of(n * BLOCK, BLOCK), BLOCK), :]
                end = w[BLOCK - 1 : BLOCK, :]
                later = prefix[0:1, :]
                tail[pl.ds(pl.multiple_of(n * BLOCK, BLOCK), BLOCK), :] = jnp.exp(end - w + later).astype(BF16)
                prefix[0:1, :] = later + end
                return 0

            lax.fori_loop(0, TOK // BLOCK, back, 0)
            dec_send[0] = jnp.broadcast_to(jnp.exp(prefix[0:1, :]), (8, 2 * KEY))

        def project(self, g, p, k):
            w, acc = bufs[g][p], (acc_a, acc_b)[p]
            u = ((z if p == 0 else y) + DELTA[k]) % 4
            if p == 0:
                lhs = xs[:, pl.ds(pl.multiple_of(u * 1024, 1024), 1024)]
            else:
                lhs = jnp.concatenate(
                    [xs[:, pl.ds(pl.multiple_of((v * 4 + u) * KB, KB), KB)] for v in range(4)], axis=1
                )
            cols = lanes[g]
            part = mm(lhs, w[pl.ds(pl.multiple_of(first_row[g][p] + u * 1024, 1024), 1024), cols])
            if k == 0:
                acc[:, cols] = part
            else:
                acc[:, cols] += part

        def key_state(self):
            def step(i, _):
                r = pl.ds(pl.multiple_of(i * 64, 64), 64)
                krows[r, :] = acc_a[r, 0:256].astype(BF16)
                vrows[r, 0:128] = acc_a[r, 256:384].astype(BF16)
                vrows[r, 128:512] = acc_b[r, 0:384].astype(BF16)
                return 0

            lax.fori_loop(0, TOK // 64, step, 0)
            k_tail = (krows[...].astype(F32) * tail[...].astype(F32)).astype(BF16)
            for h in range(2):
                kc, vc = head(h)
                s = tn(vrows[:, vc], k_tail[:, kc])
                st_send[0, vc, :] = s.astype(BF16)
            state[...] = jnp.zeros_like(state)
            prefix[0:1, :] = jnp.zeros((1, 2 * KEY), F32)

        def attend(self, lo, hi):
            def step(n, _):
                r = pl.ds(pl.multiple_of(n * BLOCK, BLOCK), BLOCK)
                row = lax.broadcasted_iota(jnp.int32, (BLOCK, BLOCK), 0)
                col = lax.broadcasted_iota(jnp.int32, (BLOCK, BLOCK), 1)
                causal = row >= col
                w = within[r, :]
                end = w[BLOCK - 1 : BLOCK, :]
                mid = end * 0.5
                q_now = jnp.concatenate([acc_a[r, 384:512], acc_b[r, 384:512]], axis=1).astype(BF16)
                q_s = q_now.astype(F32) * (KEY**-0.5) * jnp.exp(w - mid)
                k_s = krows[r, :].astype(F32) * jnp.exp(mid - w)
                e_mid = jnp.exp(mid)
                q_d = q_s * e_mid
                k_t = (k_s * e_mid).astype(BF16)
                e_end = jnp.exp(end)
                before = prefix[0:1, :]
                q_far[r, :] = (q_d * jnp.exp(before)).astype(BF16)
                prefix[0:1, :] = before + end
                q_d = q_d.astype(BF16)
                q_s = q_s.astype(BF16)
                k_s = k_s.astype(BF16)
                for h in range(2):
                    kc, vc = head(h)
                    v = vrows[r, vc]
                    scores = jnp.where(causal, nt(q_s[:, kc], k_s[:, kc]), 0.0).astype(BF16)
                    s = state[vc, :]
                    inside[r, vc] = mm(scores, v) + nt(q_d[:, kc], s.astype(BF16))
                    state[vc, :] = s * e_end[:, kc] + tn(v, k_t[:, kc])
                return 0

            lax.fori_loop(lo, hi, step, 0)

        def fold(self, total, decay, i, use):
            dec = jnp.where(use, dec_recv[i][0:1, :], 1.0)
            out_ = []
            for h in range(2):
                kc, vc = head(h)
                got = jnp.where(use, st_recv[i, vc, :].astype(F32), 0.0)
                out_.append(total[h] * dec[:, kc] + got)
            return out_, decay * dec

        def fold_y(self):
            own_decay = dec_send[0][0:1, :]
            total = [jnp.zeros((VAL, KEY), F32) for _ in range(2)]
            decay = jnp.ones((1, 2 * KEY), F32)
            for d in (3, 2, 1):
                total, decay = self.fold(total, decay, d - 1, d <= y)
            prefix[1:2, :] = decay
            for h in range(2):
                kc, vc = head(h)
                state[vc, :] = total[h]
                total[h] = total[h] * own_decay[:, kc] + st_send[0, vc, :].astype(F32)
            decay = decay * own_decay
            for d in (3, 2, 1):
                total, decay = self.fold(total, decay, d - 1, d > y)
            for h in range(2):
                kc, vc = head(h)
                st_send[1, vc, :] = total[h].astype(BF16)
            dec_send[1] = jnp.broadcast_to(decay, (8, 2 * KEY))

        def fold_z(self):
            total = [jnp.zeros((VAL, KEY), F32) for _ in range(2)]
            decay = jnp.ones((1, 2 * KEY), F32)
            for d in (3, 2, 1):
                total, decay = self.fold(total, decay, 3 + d - 1, d <= z)
            decay = prefix[1:2, :]
            for h in range(2):
                kc, vc = head(h)
                state[vc, :] = total[h] * decay[:, kc] + state[vc, :]
            hg = head_gain[...].astype(F32)

            def finish(g, _):
                r = pl.ds(pl.multiple_of(g * ROWS, 32), ROWS)
                to = self.place(g)
                for h in range(2):
                    kc, vc = head(h)
                    a = inside[r, vc] + nt(q_far[r, kc], state[vc, :].astype(BF16))
                    ms = jnp.mean(a * a, axis=-1, keepdims=True)
                    mix[to, vc] = (a * lax.rsqrt(ms + EPS) * hg[h : h + 1, :]).astype(BF16)
                return 0

            lax.fori_loop(0, 8, finish, 0)

        def place(self, g):
            mine = 1 - (g + core) % 2
            d = (g // 2 + 4 - xi) % 4
            return pl.ds(pl.multiple_of((mine * 4 + d) * ROWS, 32), ROWS)

        def gate(self, g):
            gated = gated_c if g == "c" else gated_d

            def rnd(v):
                return v.astype(BF16).astype(F32)

            def step(i, _):
                r = pl.ds(pl.multiple_of(i * 64, 64), 64)
                o = pl.ds(pl.multiple_of(i * 64 + 8, 8), 64)
                gated[o, 0:128] = rnd(rnd(acc_b[r, 256:384]) * rnd(acc_a[r, 128:256]))
                gated[o, 128:256] = rnd(rnd(acc_a[r, 0:128]) * rnd(acc_a[r, 256:384]))
                return 0

            lax.fori_loop(0, TOK // 64, step, 0)
            go(halo_copy(g))

        def rows(self, g, i):
            gated = gated_c if g == "c" else gated_d
            tp = taps[...].astype(F32)[:, slice(0, EARLY) if g == "c" else slice(EARLY, 512)]
            block = gated[pl.ds(pl.multiple_of(i * ROWS, 32), ROWS + 8), :]
            if isinstance(i, int):
                keep = jnp.where(sp == 0, 0.0, 1.0)
                rim = lax.broadcasted_iota(jnp.int32, (ROWS + 8, 1), 0) < 8
                block = jnp.where(rim, block * keep, block)
            one = pltpu.roll(block, 1, 0)[8:, :]
            two = pltpu.roll(block, 2, 0)[8:, :]
            s = tp[0:1, :] * two + tp[1:2, :] * one + tp[2:3, :] * block[8:, :]
            r = pl.ds(pl.multiple_of(i * ROWS, 32), ROWS)
            s = (s * acc_b[r, 0:256].astype(BF16).astype(F32)).astype(BF16)
            if g == "c":
                mix[self.place(i), 512:MIX] = s
            else:
                late_mix[r, :] = s

        def conv(self, g):
            def step(i, _):
                self.rows(g, i)
                return 0

            lax.fori_loop(1, 8, step, 0)

        def first_rows(self, g):
            halo_copy(g).wait_recv()
            self.rows(g, 0)

        def load_h(self):
            for c in started_q:
                c.wait_send()
            for c in h_loads():
                c.start()
            for to in (at_x(1), at_x(3), to_sib):
                pl.semaphore_signal(free_sem, inc=1, device_id=to, device_id_type=MESH)

        def start_h(self):
            for c in h_loads():
                c.wait()
            pl.semaphore_wait(free_sem, 3)

        def pair_products(self, i):
            for c in out_loads(i):
                c.wait()
            if i >= 2:
                sib_copy(i - 2).wait_send()
            sib_send[i % 2] = mm(mix[0 : 4 * ROWS, :], wo[i % 3]).astype(BF16)
            sib_copy(i).start()
            own[i % 4] = mm(mix[4 * ROWS : TOK, :], wo[i % 3])
            if i + 3 < CHUNKS:
                for c in out_loads(i + 3):
                    c.start()

        def pair(self, c, d, r0, rows):
            at = slice(d * ROWS + r0, d * ROWS + r0 + rows)
            return own[c % 4, at, :] + sib_recv[c, at, :].astype(F32)

        def far(self, c):
            sib_copy(c).wait_recv()
            for side in (0, 1):
                if c >= 4:
                    far_copy(c - 4, side).wait_send()
                far_send[c % 4, side] = self.pair(c, 2, side * 48, 48).astype(BF16)
                far_copy(c, side).start()

        def near(self, c):
            for side in (0, 1):
                d = 1 + 2 * side
                if c >= 4:
                    near_copy(c - 4, side).wait_send()
                far_copy(c, side).wait_recv()
                for half in (0, 1):
                    v = self.pair(c, d, 48 * half, 48)
                    if half == side:
                        v = v + far_recv[c, side].astype(F32)
                    near_send[c % 4, side, 48 * half : 48 * half + 48, :] = v.astype(BF16)
                near_copy(c, side).start()

        def gather(self, c):
            near_copy(c, 0).wait_recv()
            near_copy(c, 1).wait_recv()
            total = self.pair(c, 0, 0, ROWS) + near_recv[c, 0].astype(F32) + near_recv[c, 1].astype(F32)
            inside[c * ROWS : (c + 1) * ROWS, :] = total

        def exchange(self):
            for d in (1, 7, 2, 6, 3, 5, 4):
                go(late_copy(d, True))
            late_recv[t] = late_mix[pl.ds(own_rows, ROWS), :]

        def collect(self):
            for d in range(1, 8):
                late_copy(d, False).wait_recv()

        def last(self, i):
            k = slice(i * CW, (i + 1) * CW)
            lhs_f = jnp.concatenate([late_recv[g, :, 0:128] for g in range(8)], axis=1)
            lhs_h = jnp.concatenate([late_recv[g, :, 128:256] for g in range(8)], axis=1)
            w_h = jnp.concatenate([qab[g * 1024 + i * 128 : g * 1024 + (i + 1) * 128, :] for g in range(8)], axis=0)
            total = inside[i * ROWS : (i + 1) * ROWS, :] + mm(lhs_f, wf[:, k]) + mm(lhs_h, w_h)
            out[:, k] = total.astype(BF16)

        def close(self):
            for i in range(CHUNKS - 2, CHUNKS):
                sib_copy(i).wait_send()
            for i in range(CHUNKS - 4, CHUNKS):
                for side in (0, 1):
                    far_copy(i, side).wait_send()
                    near_copy(i, side).wait_send()
            for c in started:
                c.wait_send()

    device = Device()
    for kind, *what in ORDER:
        if kind == "run":
            getattr(device, what[0])(*what[1:])
        else:
            getattr(device, kind)(*what)
    device.close()


def layer(*args):
    any_ = pl.BlockSpec(memory_space=pl.ANY)
    vmem = pl.BlockSpec(memory_space=pltpu.VMEM)
    dma = pltpu.SemaphoreType.DMA

    def f32(*shape):
        return pltpu.VMEM(shape, F32)

    def bf16(*shape):
        return pltpu.VMEM(shape, BF16)

    return pl.pallas_call(
        layer_kernel,
        out_shape=jax.ShapeDtypeStruct((ROWS, MODEL), BF16),
        in_specs=[any_, vmem] + [any_] * 6 + [vmem] * 6 + [any_] * 2,
        out_specs=vmem,
        scratch_shapes=[
            bf16(TOK, MODEL),
            bf16(2 * MODEL, 512),
            bf16(MODEL, 384),
            bf16(MODEL, 384),
            bf16(MODEL, 384),
            bf16(MODEL, 384),
            bf16(8 * 128, MODEL),
            bf16(3, MIX, CW),
            f32(TOK, 512),
            f32(TOK, 512),
            bf16(TOK, 2 * KEY),
            bf16(TOK, 2 * VAL),
            bf16(TOK, 64),
            f32(TOK, 2 * KEY),
            bf16(TOK, 2 * KEY),
            f32(8, TOK),
            f32(TOK, 2 * VAL),
            bf16(TOK, 2 * KEY),
            f32(2 * VAL, KEY),
            f32(8, 2 * KEY),
            bf16(2, 2 * VAL, KEY),
            f32(2, 8, 2 * KEY),
            bf16(6, 2 * VAL, KEY),
            f32(6, 8, 2 * KEY),
            f32(TOK + 8, EARLY),
            f32(TOK + 8, LATE),
            bf16(TOK, MIX),
            bf16(TOK, LATE),
            bf16(8, ROWS, LATE),
            f32(4, 4 * ROWS, CW),
            bf16(2, 4 * ROWS, CW),
            bf16(CHUNKS, 4 * ROWS, CW),
            bf16(4, 2, 48, CW),
            bf16(CHUNKS, 2, 48, CW),
            bf16(4, 2, ROWS, CW),
            bf16(CHUNKS, 2, ROWS, CW),
            dma((22,)),
            dma((2 * CHUNKS,)),
            dma((8, 20)),
            dma((8, 20)),
            dma((30,)),
            dma((30,)),
            dma((16,)),
            dma((16,)),
            dma((2,)),
            dma((2,)),
            dma((7,)),
            dma((7,)),
            dma((CHUNKS,)),
            dma((CHUNKS,)),
            dma((CHUNKS, 2)),
            dma((CHUNKS, 2)),
            dma((CHUNKS, 2)),
            dma((CHUNKS, 2)),
            pltpu.SemaphoreType.REGULAR,
        ],
        compiler_params=pltpu.CompilerParams(
            collective_id=0, has_side_effects=True, vmem_limit_bytes=67_000_000
        ),
        name="layer",
    )(*args)


def body(
    hidden_activations,
    entry_rescale_vector,
    probe_matrix,
    lookup_address_matrix,
    payload_matrix,
    postfilter_switch_matrix,
    prefilter_switch_matrix,
    filter_source_matrix,
    forget_left_factor,
    forget_right_factor,
    forget_offset_per_feature,
    forget_spike_additions,
    subspace_rescale_vector,
    depthwise_filter_taps,
    mixer_result_matrix,
    filter_result_matrix,
):
    return layer(
        hidden_activations,
        entry_rescale_vector.reshape(32, 128),
        probe_matrix,
        lookup_address_matrix,
        payload_matrix,
        postfilter_switch_matrix,
        prefilter_switch_matrix,
        filter_source_matrix,
        forget_left_factor.T,
        forget_right_factor,
        forget_offset_per_feature[None, :],
        forget_spike_additions,
        subspace_rescale_vector,
        depthwise_filter_taps,
        mixer_result_matrix,
        filter_result_matrix,
    )


def solution(mesh):
    split = Mesh(mesh.devices.reshape(4, 4, mesh.shape["tp"]), ("sp_0", "sp_1", "tp"))
    in_specs = (
        P(SP_TP, None),
        P(),
        P(SP, "tp"),
        P(SP, "tp"),
        P(SP, "tp"),
        P(SP, "tp"),
        P(SP, "tp"),
        P(SP, "tp"),
        P(),
        P(None, "tp"),
        P("tp"),
        P("tp", SP),
        P("tp", None),
        P(None, "tp"),
        P("tp", None),
        P("tp", None),
    )
    out_specs = P(SP_TP, None)
    return jax.shard_map(body, mesh=split, in_specs=in_specs, out_specs=out_specs, check_vma=False)
```

```python
import jax
import jax.numpy as jnp
from jax import lax
from jax.experimental import pallas as pl
from jax.experimental.pallas import tpu as pltpu
from jax.sharding import Mesh
from jax.sharding import PartitionSpec as P

MESH = pl.DeviceIdType.MESH
SP = ("sp_0", "sp_1")
SP_TP = ("sp_0", "sp_1", "tp")
F32 = jnp.float32
BF16 = jnp.bfloat16
HIGHEST = lax.Precision.HIGHEST

BLOCK = 64
ROWS = 96
TOK = 768
MODEL = 4096
KB = 256
LATE = 256
EARLY = 512 - LATE
MIX = 512 + EARLY
CHUNKS = 8
CW = MODEL // CHUNKS
KEY, VAL = 128, 256
EPS = 1e-06
DELTA = (0, 3, 1, 2)


def nt(a, b):
    return lax.dot_general(a, b, (((1,), (1,)), ((), ())), preferred_element_type=F32)


def tn(a, b):
    return lax.dot_general(a, b, (((0,), (0,)), ((), ())), preferred_element_type=F32)


def mm(a, b):
    return jnp.dot(a, b, preferred_element_type=F32)


SEND, WAIT, RUN = "send", "wait", "run"
W, R, S = "w", "r", "s"
Q, E, C, D = "q", "e", "c", "d"
X, F, H = "x", "f", "h"
T_NORM = "norm"
T_LOW_RANK = "low_rank"
T_RATE = "rate"
T_SUFFIX = "suffix"
T_PROJECT = "project"
T_KEY_STATE = "key_state"
T_ATTEND = "attend"
T_FOLD_Y = "fold_y"
T_FOLD_Z = "fold_z"
T_GATE = "gate"
T_CONV = "conv"
T_FIRST_ROWS = "first_rows"
T_EXCHANGE = "exchange"
T_LOAD_H = "load_h"
T_START_H = "start_h"
T_PAIR_PRODUCTS = "pair_products"
T_FAR = "far"
T_NEAR = "near"
T_GATHER = "gather"
T_COLLECT = "collect"
T_LAST = "last"
ORDER = (
    (SEND, W, Q, 0, 0), (SEND, W, Q, 1, 4), (SEND, W, Q, 0, 1), (SEND, W, Q, 1, 5), (SEND, W, Q, 1, 0),
    (SEND, W, Q, 0, 4), (SEND, W, Q, 1, 1), (SEND, W, Q, 0, 5), (SEND, R, F, 6), (RUN, T_NORM), (SEND, R, X, 0),
    (SEND, R, X, 2), (SEND, R, X, 6), (SEND, W, E, 0, 0), (SEND, W, E, 0, 1), (SEND, W, E, 1, 0),
    (SEND, W, E, 1, 1), (SEND, W, E, 0, 4), (SEND, W, E, 0, 5), (SEND, W, E, 1, 4), (SEND, W, E, 1, 5),
    (SEND, R, X, 1), (SEND, R, X, 3), (WAIT, W, Q, 0, 0), (SEND, W, Q, 0, 2), (WAIT, W, Q, 0, 1),
    (SEND, W, Q, 0, 3), (WAIT, W, Q, 1, 0), (SEND, W, Q, 1, 2), (WAIT, W, Q, 1, 1), (SEND, W, Q, 1, 3),
    (SEND, W, Q, 0, 6), (SEND, W, Q, 0, 7), (SEND, W, Q, 1, 6), (SEND, W, Q, 1, 7), (SEND, W, Q, 0, 8),
    (SEND, W, Q, 0, 9), (SEND, W, Q, 1, 8), (SEND, W, Q, 1, 9), (WAIT, R, X, 0), (SEND, R, X, 4),
    (WAIT, R, X, 2), (SEND, R, X, 5), (WAIT, W, Q, 0, 2), (WAIT, W, Q, 0, 3), (SEND, W, Q, 0, 10),
    (SEND, W, Q, 0, 11), (WAIT, W, Q, 1, 2), (WAIT, W, Q, 1, 3), (SEND, W, Q, 1, 10), (SEND, W, Q, 1, 11),
    (WAIT, R, X, 1), (SEND, R, X, 7), (WAIT, R, X, 3), (SEND, R, X, 8), (WAIT, W, Q, 0, 6), (SEND, W, Q, 0, 14),
    (WAIT, W, Q, 0, 7), (SEND, W, Q, 0, 15), (WAIT, W, Q, 1, 6), (SEND, W, Q, 1, 14), (WAIT, W, Q, 1, 7),
    (SEND, W, Q, 1, 15), (SEND, R, F, 0), (SEND, R, F, 2), (WAIT, W, Q, 0, 8), (SEND, W, Q, 0, 16),
    (WAIT, W, Q, 0, 9), (SEND, W, Q, 0, 17), (WAIT, W, Q, 1, 8), (SEND, W, Q, 1, 16), (WAIT, W, Q, 1, 9),
    (SEND, W, Q, 1, 17), (WAIT, W, Q, 0, 4), (SEND, W, Q, 0, 12), (WAIT, W, Q, 0, 5), (SEND, W, Q, 0, 13),
    (WAIT, W, Q, 1, 4), (SEND, W, Q, 1, 12), (WAIT, W, Q, 1, 5), (SEND, W, Q, 1, 13), (WAIT, W, Q, 0, 10),
    (SEND, W, Q, 0, 18), (WAIT, W, Q, 0, 11), (SEND, W, Q, 0, 19), (WAIT, W, Q, 1, 10), (SEND, W, Q, 1, 18),
    (WAIT, W, Q, 1, 11), (SEND, W, Q, 1, 19), (WAIT, R, X, 4), (WAIT, R, X, 5), (SEND, R, X, 9),
    (WAIT, W, E, 0, 0), (SEND, W, E, 0, 2), (WAIT, W, E, 0, 1), (SEND, W, E, 0, 3), (WAIT, W, E, 1, 0),
    (SEND, W, E, 1, 2), (WAIT, W, E, 1, 1), (SEND, W, E, 1, 3), (SEND, W, E, 0, 8), (SEND, W, E, 0, 9),
    (SEND, W, E, 1, 8), (SEND, W, E, 1, 9), (SEND, W, E, 0, 6), (SEND, W, E, 0, 7), (SEND, W, E, 1, 6),
    (SEND, W, E, 1, 7), (WAIT, W, E, 0, 4), (SEND, W, E, 0, 12), (WAIT, W, E, 0, 5), (SEND, W, E, 0, 13),
    (WAIT, W, E, 1, 4), (SEND, W, E, 1, 12), (WAIT, W, E, 1, 5), (SEND, W, E, 1, 13), (WAIT, R, X, 6),
    (WAIT, R, X, 7), (WAIT, R, X, 8), (WAIT, R, X, 9), (RUN, T_LOW_RANK), (SEND, W, C, 0, 0),
    (SEND, W, C, 0, 1), (SEND, W, C, 1, 0), (SEND, W, C, 1, 1), (SEND, R, F, 1), (SEND, R, F, 3),
    (RUN, T_RATE, 0, 2), (RUN, T_RATE, 2, 4), (RUN, T_RATE, 4, 6), (WAIT, W, E, 0, 2), (WAIT, W, E, 0, 3),
    (SEND, W, E, 0, 10), (SEND, W, E, 0, 11), (WAIT, W, E, 1, 2), (WAIT, W, E, 1, 3), (SEND, W, E, 1, 10),
    (SEND, W, E, 1, 11), (RUN, T_SUFFIX), (WAIT, W, Q, 0, 12), (WAIT, W, Q, 0, 13), (RUN, T_PROJECT, Q, 0, 0),
    (WAIT, W, E, 0, 6), (SEND, W, E, 0, 14), (WAIT, W, E, 0, 8), (SEND, W, E, 0, 16), (WAIT, W, E, 0, 7),
    (SEND, W, E, 0, 15), (WAIT, W, E, 0, 9), (SEND, W, E, 0, 17), (WAIT, W, E, 1, 6), (SEND, W, E, 1, 14),
    (WAIT, W, E, 1, 8), (SEND, W, E, 1, 16), (WAIT, W, E, 1, 7), (SEND, W, E, 1, 15), (WAIT, W, E, 1, 9),
    (SEND, W, E, 1, 17), (WAIT, W, Q, 0, 14), (WAIT, W, Q, 0, 15), (RUN, T_PROJECT, Q, 0, 1),
    (SEND, W, C, 0, 4), (SEND, W, C, 0, 5), (SEND, W, C, 1, 4), (SEND, W, C, 1, 5), (WAIT, W, Q, 0, 16),
    (WAIT, W, Q, 0, 17), (RUN, T_PROJECT, Q, 0, 2), (WAIT, W, Q, 0, 18), (WAIT, W, Q, 0, 19),
    (RUN, T_PROJECT, Q, 0, 3), (WAIT, W, Q, 1, 12), (WAIT, W, Q, 1, 13), (RUN, T_PROJECT, Q, 1, 0),
    (WAIT, W, Q, 1, 14), (WAIT, W, Q, 1, 15), (RUN, T_PROJECT, Q, 1, 1), (WAIT, W, Q, 1, 16),
    (WAIT, W, Q, 1, 17), (RUN, T_PROJECT, Q, 1, 2), (WAIT, W, C, 0, 0), (SEND, W, C, 0, 2), (WAIT, W, C, 0, 1),
    (SEND, W, C, 0, 3), (WAIT, W, C, 1, 0), (SEND, W, C, 1, 2), (WAIT, W, C, 1, 1), (SEND, W, C, 1, 3),
    (WAIT, R, F, 0), (SEND, R, F, 4), (WAIT, R, F, 2), (SEND, R, F, 5), (WAIT, W, Q, 1, 18),
    (WAIT, W, Q, 1, 19), (RUN, T_PROJECT, Q, 1, 3), (WAIT, W, E, 0, 10), (SEND, W, E, 0, 18),
    (WAIT, W, E, 0, 11), (SEND, W, E, 0, 19), (WAIT, W, E, 1, 10), (SEND, W, E, 1, 18), (WAIT, W, E, 1, 11),
    (SEND, W, E, 1, 19), (RUN, T_KEY_STATE), (SEND, S, 0, 0), (SEND, S, 0, 1), (SEND, W, C, 1, 6),
    (SEND, W, C, 1, 7), (WAIT, W, E, 0, 12), (WAIT, W, E, 0, 13), (RUN, T_PROJECT, E, 0, 0),
    (WAIT, W, E, 0, 14), (WAIT, W, E, 0, 15), (RUN, T_PROJECT, E, 0, 1), (WAIT, W, E, 0, 16),
    (WAIT, W, E, 0, 17), (RUN, T_PROJECT, E, 0, 2), (WAIT, W, E, 1, 12), (WAIT, W, E, 1, 13),
    (RUN, T_PROJECT, E, 1, 0), (WAIT, W, E, 1, 14), (WAIT, W, E, 1, 15), (RUN, T_PROJECT, E, 1, 1),
    (SEND, W, C, 0, 6), (SEND, W, C, 0, 7), (WAIT, W, E, 1, 16), (WAIT, W, E, 1, 17), (RUN, T_PROJECT, E, 1, 2),
    (WAIT, R, F, 1), (SEND, R, F, 7), (WAIT, R, F, 3), (SEND, R, F, 8), (WAIT, W, C, 1, 4), (SEND, W, C, 1, 12),
    (WAIT, W, C, 1, 5), (SEND, W, C, 1, 13), (WAIT, W, C, 1, 2), (WAIT, W, C, 1, 3), (SEND, W, C, 1, 10),
    (SEND, W, C, 1, 11), (WAIT, W, E, 0, 18), (WAIT, W, E, 0, 19), (RUN, T_PROJECT, E, 0, 3),
    (WAIT, W, C, 0, 2), (WAIT, W, C, 0, 3), (SEND, W, C, 0, 10), (SEND, W, C, 0, 11), (WAIT, W, E, 1, 18),
    (WAIT, W, E, 1, 19), (RUN, T_PROJECT, E, 1, 3), (RUN, T_LOAD_H), (RUN, T_ATTEND, 0, 3),
    (RUN, T_ATTEND, 3, 6), (RUN, T_ATTEND, 6, 9), (RUN, T_START_H), (SEND, R, H, 6), (WAIT, S, 0, 0),
    (SEND, S, 0, 2), (WAIT, S, 0, 1), (SEND, S, 0, 3), (WAIT, W, C, 1, 6), (SEND, W, C, 1, 14),
    (WAIT, W, C, 1, 7), (SEND, W, C, 1, 15), (SEND, R, H, 0), (SEND, R, H, 2), (RUN, T_ATTEND, 9, 12),
    (WAIT, W, C, 0, 4), (SEND, W, C, 0, 12), (WAIT, W, C, 0, 5), (SEND, W, C, 0, 13), (SEND, W, C, 1, 8),
    (SEND, W, C, 1, 9), (WAIT, W, C, 1, 12), (WAIT, W, C, 1, 13), (RUN, T_PROJECT, C, 1, 0), (WAIT, W, C, 0, 6),
    (SEND, W, C, 0, 14), (WAIT, W, C, 0, 7), (SEND, W, C, 0, 15), (WAIT, R, F, 4), (WAIT, R, F, 5),
    (SEND, R, F, 9), (SEND, W, C, 0, 8), (SEND, W, C, 0, 9), (WAIT, W, C, 1, 10), (SEND, W, C, 1, 18),
    (WAIT, W, C, 1, 11), (SEND, W, C, 1, 19), (SEND, W, D, 1, 4), (SEND, W, D, 1, 5), (WAIT, W, C, 1, 14),
    (WAIT, W, C, 1, 15), (RUN, T_PROJECT, C, 1, 1), (SEND, R, H, 1), (SEND, R, H, 3), (WAIT, S, 0, 2),
    (WAIT, S, 0, 3), (RUN, T_FOLD_Y), (WAIT, W, C, 0, 10), (SEND, W, C, 0, 18), (WAIT, W, C, 0, 11),
    (SEND, W, C, 0, 19), (WAIT, W, C, 0, 12), (WAIT, W, C, 0, 13), (RUN, T_PROJECT, C, 0, 0), (SEND, S, 1, 0),
    (SEND, S, 1, 1), (SEND, W, D, 0, 4), (SEND, W, D, 0, 5), (WAIT, W, C, 0, 14), (WAIT, W, C, 0, 15),
    (RUN, T_PROJECT, C, 0, 1), (WAIT, W, C, 1, 8), (SEND, W, C, 1, 16), (WAIT, W, C, 1, 9), (SEND, W, C, 1, 17),
    (WAIT, W, C, 0, 8), (SEND, W, C, 0, 16), (WAIT, W, C, 0, 9), (SEND, W, C, 0, 17), (SEND, W, D, 0, 0),
    (SEND, W, D, 0, 1), (SEND, W, D, 1, 0), (SEND, W, D, 1, 1), (WAIT, R, H, 0), (SEND, R, H, 4),
    (WAIT, R, H, 2), (SEND, R, H, 5), (WAIT, S, 1, 0), (SEND, S, 1, 2), (WAIT, S, 1, 1), (SEND, S, 1, 3),
    (WAIT, W, D, 0, 4), (SEND, W, D, 0, 12), (WAIT, W, D, 0, 5), (SEND, W, D, 0, 13), (WAIT, W, D, 1, 4),
    (SEND, W, D, 1, 12), (WAIT, W, D, 1, 5), (SEND, W, D, 1, 13), (WAIT, W, C, 1, 16), (WAIT, W, C, 1, 17),
    (RUN, T_PROJECT, C, 1, 2), (WAIT, W, C, 1, 18), (WAIT, W, C, 1, 19), (RUN, T_PROJECT, C, 1, 3),
    (WAIT, W, C, 0, 16), (WAIT, W, C, 0, 17), (RUN, T_PROJECT, C, 0, 2), (WAIT, W, C, 0, 18),
    (WAIT, W, C, 0, 19), (RUN, T_PROJECT, C, 0, 3), (WAIT, R, H, 1), (SEND, R, H, 7), (WAIT, R, H, 3),
    (SEND, R, H, 8), (RUN, T_GATE, C), (RUN, T_CONV, C), (WAIT, W, D, 0, 0), (SEND, W, D, 0, 2),
    (WAIT, W, D, 0, 1), (SEND, W, D, 0, 3), (SEND, W, D, 0, 6), (SEND, W, D, 0, 7), (WAIT, W, D, 1, 0),
    (SEND, W, D, 1, 6), (SEND, W, D, 1, 7), (SEND, W, D, 1, 2), (WAIT, W, D, 1, 1), (SEND, W, D, 1, 3),
    (WAIT, S, 1, 2), (WAIT, S, 1, 3), (RUN, T_FOLD_Z), (RUN, T_FIRST_ROWS, C), (RUN, T_PAIR_PRODUCTS, 0),
    (SEND, W, D, 0, 8), (SEND, W, D, 0, 9), (SEND, W, D, 1, 8), (SEND, W, D, 1, 9), (RUN, T_PAIR_PRODUCTS, 1),
    (RUN, T_PAIR_PRODUCTS, 2), (RUN, T_PAIR_PRODUCTS, 3), (RUN, T_FAR, 0), (WAIT, W, D, 0, 12),
    (WAIT, W, D, 0, 13), (RUN, T_PROJECT, D, 0, 0), (RUN, T_FAR, 1), (WAIT, W, D, 1, 12), (WAIT, W, D, 1, 13),
    (RUN, T_PROJECT, D, 1, 0), (RUN, T_FAR, 2), (WAIT, W, D, 0, 6), (SEND, W, D, 0, 14), (WAIT, W, D, 0, 7),
    (SEND, W, D, 0, 15), (RUN, T_FAR, 3), (WAIT, W, D, 1, 6), (SEND, W, D, 1, 14), (WAIT, W, D, 1, 7),
    (SEND, W, D, 1, 15), (WAIT, W, D, 0, 2), (WAIT, W, D, 0, 3), (SEND, W, D, 0, 10), (SEND, W, D, 0, 11),
    (WAIT, W, D, 1, 2), (WAIT, W, D, 1, 3), (SEND, W, D, 1, 10), (SEND, W, D, 1, 11), (WAIT, R, H, 4),
    (WAIT, R, H, 5), (SEND, R, H, 9), (RUN, T_NEAR, 0), (RUN, T_NEAR, 1), (RUN, T_NEAR, 2), (WAIT, W, D, 0, 8),
    (SEND, W, D, 0, 16), (WAIT, W, D, 0, 9), (SEND, W, D, 0, 17), (WAIT, W, D, 1, 8), (SEND, W, D, 1, 16),
    (WAIT, W, D, 1, 9), (SEND, W, D, 1, 17), (RUN, T_NEAR, 3), (WAIT, W, D, 0, 14), (WAIT, W, D, 0, 15),
    (RUN, T_PROJECT, D, 0, 1), (RUN, T_GATHER, 0), (RUN, T_PAIR_PRODUCTS, 4), (WAIT, W, D, 1, 14),
    (WAIT, W, D, 1, 15), (RUN, T_PROJECT, D, 1, 1), (RUN, T_GATHER, 1), (RUN, T_PAIR_PRODUCTS, 5),
    (RUN, T_FAR, 4), (WAIT, W, D, 0, 10), (SEND, W, D, 0, 18), (WAIT, W, D, 0, 11), (SEND, W, D, 0, 19),
    (WAIT, W, D, 1, 10), (SEND, W, D, 1, 18), (WAIT, W, D, 1, 11), (SEND, W, D, 1, 19), (RUN, T_GATHER, 2),
    (RUN, T_PAIR_PRODUCTS, 6), (RUN, T_FAR, 5), (WAIT, W, D, 0, 16), (WAIT, W, D, 0, 17),
    (RUN, T_PROJECT, D, 0, 2), (RUN, T_GATHER, 3), (RUN, T_FAR, 6), (RUN, T_PAIR_PRODUCTS, 7), (RUN, T_NEAR, 4),
    (WAIT, W, D, 1, 16), (WAIT, W, D, 1, 17), (RUN, T_PROJECT, D, 1, 2), (RUN, T_NEAR, 5), (WAIT, W, D, 0, 18),
    (WAIT, W, D, 0, 19), (RUN, T_PROJECT, D, 0, 3), (RUN, T_FAR, 7), (WAIT, W, D, 1, 18), (WAIT, W, D, 1, 19),
    (RUN, T_PROJECT, D, 1, 3), (RUN, T_GATE, D), (RUN, T_NEAR, 6), (RUN, T_CONV, D), (RUN, T_GATHER, 4),
    (RUN, T_FIRST_ROWS, D), (RUN, T_EXCHANGE), (RUN, T_GATHER, 5), (RUN, T_NEAR, 7), (RUN, T_GATHER, 6),
    (WAIT, R, F, 6), (WAIT, R, F, 7), (WAIT, R, F, 8), (WAIT, R, F, 9), (WAIT, R, H, 6), (WAIT, R, H, 7),
    (WAIT, R, H, 8), (WAIT, R, H, 9), (RUN, T_COLLECT), (RUN, T_LAST, 0), (RUN, T_LAST, 1), (RUN, T_LAST, 2),
    (RUN, T_LAST, 3), (RUN, T_LAST, 4), (RUN, T_GATHER, 7), (RUN, T_LAST, 5), (RUN, T_LAST, 6),
    (RUN, T_LAST, 7),
)


def layer_kernel(
    x_in,
    gain,
    w_q,
    w_k,
    w_v,
    w_out,
    w_in,
    w_src,
    left,
    right,
    offset,
    spikes,
    head_gain,
    taps,
    w_a,
    w_c,
    out,
    xs,
    qab,
    ca,
    cb,
    da,
    db,
    wf,
    wo,
    acc_a,
    acc_b,
    krows,
    vrows,
    low,
    within,
    tail,
    spk,
    inside,
    q_far,
    state,
    prefix,
    st_send,
    dec_send,
    st_recv,
    dec_recv,
    gated_c,
    gated_d,
    mix,
    late_mix,
    late_recv,
    own,
    sib_send,
    sib_recv,
    far_send,
    far_recv,
    near_send,
    near_recv,
    load_sem,
    out_sem,
    w_send,
    w_recv,
    x_send,
    x_recv,
    s_send,
    s_recv,
    h_send,
    h_recv,
    e_send,
    e_recv,
    ss,
    sr,
    fs,
    fr,
    ns,
    nr,
    free_sem,
):
    z = lax.axis_index("sp_0")
    y = lax.axis_index("sp_1")
    t = lax.axis_index("tp")
    core = t % 2
    xi = t // 2
    sp = z * 4 + y
    sp_next = (sp + 1) % 16
    sp_prev = (sp + 15) % 16
    to_next = {"sp_0": sp_next // 4, "sp_1": sp_next % 4}
    to_prev = {"sp_0": sp_prev // 4, "sp_1": sp_prev % 4}
    to_sib = {"tp": xi * 2 + (1 - core)}

    def at_z(d):
        return {"sp_0": (z + d) % 4}

    def at_y(d):
        return {"sp_1": (y + d) % 4}

    def at_x(d):
        return {"tp": ((xi + d) % 4) * 2 + core}

    def remote(ref, dst, sems, at, to):
        return pltpu.make_async_remote_copy(
            src_ref=ref,
            dst_ref=dst,
            send_sem=sems[0].at[at],
            recv_sem=sems[1].at[at],
            device_id=to,
            device_id_type=MESH,
        )

    own0 = pl.ds(pl.multiple_of(sp * KB, KB), KB)
    own1 = pl.ds(pl.multiple_of((y * 4 + z) * KB, KB), KB)
    own1_v = pl.ds(pl.multiple_of(MODEL + (y * 4 + z) * KB, KB), KB)
    own_rows = pl.multiple_of(t * ROWS, 32)
    loads = [
        (x_in, xs.at[pl.ds(own_rows, ROWS), :]),
        (w_k, qab.at[own0, 0:256]),
        (w_v.at[:, 0:128], qab.at[own0, 256:384]),
        (w_q.at[:, 0:128], qab.at[own0, 384:512]),
        (w_v.at[:, 128:512], qab.at[own1_v, 0:384]),
        (w_q.at[:, 128:256], qab.at[own1_v, 384:512]),
        (w_in.at[:, 128:256], ca.at[own0, 0:128]),
        (w_src.at[:, 0:256], ca.at[own0, 128:384]),
        (w_out.at[:, 0:256], cb.at[own1, 0:256]),
        (w_in.at[:, 0:128], cb.at[own1, 256:384]),
        (w_in.at[:, 384:512], da.at[own0, 0:128]),
        (w_src.at[:, 256:512], da.at[own0, 128:384]),
        (w_out.at[:, 256:512], db.at[own1, 0:256]),
        (w_in.at[:, 256:384], db.at[own1, 256:384]),
        (w_c.at[EARLY : EARLY + 128, :], wf.at[pl.ds(pl.multiple_of(t * 128, 128), 128), :]),
    ]
    loads = [pltpu.make_async_copy(a, b, load_sem.at[i]) for i, (a, b) in enumerate(loads)]
    for c in loads:
        c.start()

    barrier = pltpu.get_barrier_semaphore()
    peers = [at_z(1), at_z(3), at_y(1), at_y(3), to_next, to_prev] + [{"tp": (t + d) % 8} for d in range(1, 8)]
    for p in peers:
        pl.semaphore_signal(barrier, inc=1, device_id=p, device_id_type=MESH)

    def h_loads():
        return [
            pltpu.make_async_copy(
                w_c.at[EARLY + 128 : 512, pl.ds(i * 512, 512)],
                qab.at[pl.ds(pl.multiple_of(t * 1024 + i * 128, 128), 128), :],
                load_sem.at[15 + i],
            )
            for i in range(8)
        ]

    def out_loads(i):
        cols = pl.ds(i * CW, CW)
        return (
            pltpu.make_async_copy(w_a.at[:, cols], wo.at[i % 3, 0:512, :], out_sem.at[2 * i]),
            pltpu.make_async_copy(w_c.at[0:EARLY, cols], wo.at[i % 3, 512:MIX, :], out_sem.at[2 * i + 1]),
        )

    pl.semaphore_wait(barrier, len(peers))

    started = []
    started_q = []

    def go(c, group=None):
        c.start()
        (started_q if group in ("q", "e") else started).append(c)

    bufs = {"q": (qab, qab), "e": (qab, qab), "c": (ca, cb), "d": (da, db)}
    first_row = {"q": (0, MODEL), "e": (0, MODEL), "c": (0, 0), "d": (0, 0)}
    lanes = {"q": slice(0, 384), "e": slice(384, 512), "c": slice(0, 384), "d": slice(0, 384)}
    base = {"q": 0, "c": 2, "d": 4, "e": 6}
    rings = {"x": (xs, ROWS, 0), "f": (wf, 128, 10), "h": (qab, 1024, 20)}
    xm, xp, xf = (xi + 3) % 4, (xi + 1) % 4, (xi + 2) % 4

    def w_copy(g, path, slot, du, dv, axis, step, row=0, rows=KB):
        u0, v0 = (z, y) if path == 0 else (y, z)
        j = ((u0 + du) % 4) * 4 + (v0 + dv) % 4
        ref = bufs[g][path].at[pl.ds(pl.multiple_of(first_row[g][path] + j * KB + row, 128), rows), lanes[g]]
        to = at_z(step) if (axis == 0) == (path == 0) else at_y(step)
        return remote(ref, ref, (w_send, w_recv), (base[g] + path, slot), to)

    def ring_copy(n, slot, x_from, top, halves, to, c=None):
        buf, rows, first = rings[n]
        half = rows // 2
        at = (x_from * 2 + (core if c is None else c)) * rows + (0 if top else half)
        ref = buf.at[pl.ds(pl.multiple_of(at, 16), half * halves), :]
        return remote(ref, ref, (x_send, x_recv), first + slot, to)

    right_x, left_x = at_x(1), at_x(3)

    def st_copy(ph, slot):
        to = (at_y if ph == 0 else at_z)(1 if slot % 2 == 0 else 3)
        i = ph * 3
        if slot < 2:
            a, b = st_send.at[ph], st_recv.at[i + 2 * slot]
        else:
            half = pl.ds((slot - 2) * VAL, VAL)
            a, b = st_recv.at[i + 2 * (slot - 2), half, :], st_recv.at[i + 1, half, :]
        return remote(a, b, (s_send, s_recv), ph * 8 + slot, to)

    def dec_copy(ph, slot):
        to = (at_y if ph == 0 else at_z)(1 if slot != 1 else 3)
        i = ph * 3
        if slot < 2:
            a, b = dec_send.at[ph], dec_recv.at[i + 2 * slot]
        else:
            a, b = dec_recv.at[i], dec_recv.at[i + 1]
        return remote(a, b, (s_send, s_recv), ph * 8 + 4 + slot, to)

    def halo_copy(g):
        buf = gated_c if g == "c" else gated_d
        i = 0 if g == "c" else 1
        return remote(buf.at[pl.ds(TOK, 8), :], buf.at[pl.ds(0, 8), :], (h_send, h_recv), i, to_next)

    def sib_copy(c):
        return remote(sib_send.at[c % 2], sib_recv.at[c], (ss, sr), c, to_sib)

    def far_copy(c, side):
        return remote(far_send.at[c % 4, side], far_recv.at[c, side], (fs, fr), (c, side), right_x if side == 0 else left_x)

    def near_copy(c, side):
        return remote(near_send.at[c % 4, side], near_recv.at[c, side], (ns, nr), (c, side), right_x if side == 0 else left_x)

    def late_copy(d, sending):
        g = (t + d) % 8
        me = t if sending else (t + 8 - d) % 8
        src = late_mix.at[pl.ds(pl.multiple_of(g * ROWS, 32), ROWS), :]
        return remote(src, late_recv.at[me], (e_send, e_recv), d - 1, {"tp": g})

    def w_sent(g, p, slot):
        if slot < 2:
            return w_copy(g, p, slot, 0, 0, 0, 1 + 2 * slot)
        if slot < 4:
            return w_copy(g, p, slot, 3 if slot == 2 else 1, 0, 0, 1 if slot == 2 else 3, 128 * (slot - 2), 128)
        k, side = DELTA[(slot - 4) % 8 // 2], slot % 2
        if slot < 12:
            return w_copy(g, p, slot, k, 0, 1, 1 + 2 * side)
        return w_copy(g, p, slot, k, 1 if side else 3, 1, 1 + 2 * side, 128 * side, 128)

    def w_came(g, p, slot):
        side = slot % 2
        step, row = 1 + 2 * side, 128 * side
        if slot < 2:
            return w_copy(g, p, slot, 1 if side else 3, 0, 0, step)
        if slot < 4:
            return w_copy(g, p, slot, 2, 0, 0, step, row, 128)
        k = DELTA[(slot - 4) % 8 // 2]
        if slot < 12:
            return w_copy(g, p, slot, k, 1 if side else 3, 1, step)
        return w_copy(g, p, slot, k, 2, 1, step, row, 128)

    waiting = {"q": (1, 2, 4), "e": (3, 5), "c": (6, 7, 8, 9), "d": (10, 11, 12, 13), "f": (14,)}

    ring_sent = (
        (0, True, 1, 1), (0, False, 1, 1), (0, False, 1, 3), (0, True, 1, 3), (3, True, 1, 1), (1, False, 1, 3),
        (0, True, 2, 0), (3, True, 2, 0), (1, True, 2, 0), (2, True, 2, 0),
    )
    ring_came = (
        (3, True, 1, 1), (3, False, 1, 1), (1, False, 1, 3), (1, True, 1, 3), (2, True, 1, 1), (2, False, 1, 3),
        (0, True, 2, 0), (3, True, 2, 0), (1, True, 2, 0), (2, True, 2, 0),
    )

    def ring(n, slot, came):
        d, top, halves, step = (ring_came if came else ring_sent)[slot]
        to = to_sib if step == 0 else at_x(step)
        other = came and step == 0
        return ring_copy(n, slot, (xi + d) % 4, top, halves, to, 1 - core if other else None)

    def head(h):
        return slice(h * KEY, (h + 1) * KEY), slice(h * VAL, (h + 1) * VAL)

    class Device:
        def send(self, kind, *a):
            for i in waiting.pop(a[0], ()):
                loads[i].wait()
            if kind == "w":
                go(w_sent(*a), a[0])
            elif kind == "r":
                go(ring(*a, False))
            else:
                go(st_copy(*a))
                if a[1] < 3:
                    go(dec_copy(*a))

        def wait(self, kind, *a):
            if kind == "w":
                w_came(*a).wait_recv()
            elif kind == "r":
                ring(*a, True).wait_recv()
            elif kind == "s":
                st_copy(*a).wait_recv()
                if a[1] < 3:
                    dec_copy(*a).wait_recv()

        def norm(self):
            loads[0].wait()

            def step(i, _):
                r = pl.ds(pl.multiple_of(own_rows + i * 16, 16), 16)
                v = xs[r, :].astype(F32)
                inv = lax.rsqrt(jnp.mean(v * v, axis=-1, keepdims=True) + EPS)
                g = gain[...].astype(F32)
                for c in range(32):
                    k = slice(c * 128, (c + 1) * 128)
                    xs[r, k] = (v[:, k] * inv * g[c : c + 1, :]).astype(BF16)
                return 0

            lax.fori_loop(0, ROWS // 16, step, 0)
            spk[...] = jnp.zeros_like(spk)
            spk[0:2, :] = spikes[...]
            for i in range(3):
                for c in out_loads(i):
                    c.start()

        def low_rank(self):
            low[...] = nt(xs[...], left[...]).astype(BF16)

        def rate(self, lo, hi):
            lane_head = lax.broadcasted_iota(jnp.int32, (8, 2 * KEY), 1) // KEY
            pick = jnp.where(lax.broadcasted_iota(jnp.int32, (8, 2 * KEY), 0) == lane_head, 1.0, 0.0).astype(F32)
            row = lax.broadcasted_iota(jnp.int32, (128, 128), 0)
            col = lax.broadcasted_iota(jnp.int32, (128, 128), 1)
            low_tri = jnp.where((row >= col) & (row // BLOCK == col // BLOCK), 1.0, 0.0).astype(F32)

            def step(i, _):
                r = pl.ds(pl.multiple_of(i * 128, 128), 128)
                g = mm(low[r, :], right[...]) + offset[...]
                ls = jnp.minimum(g, 0.0) - jnp.log1p(jnp.exp(-jnp.abs(g)))
                spike = lax.dot_general(
                    spk[:, r], pick, (((0,), (0,)), ((), ())), precision=HIGHEST, preferred_element_type=F32
                )
                within[r, :] = jnp.dot(
                    low_tri, ls * (1.0 / 16.0) + spike, precision=HIGHEST, preferred_element_type=F32
                )
                return 0

            lax.fori_loop(lo, hi, step, 0)

        def suffix(self):
            prefix[0:1, :] = jnp.zeros((1, 2 * KEY), F32)

            def back(i, _):
                n = TOK // BLOCK - 1 - i
                w = within[pl.ds(pl.multiple_of(n * BLOCK, BLOCK), BLOCK), :]
                end = w[BLOCK - 1 : BLOCK, :]
                later = prefix[0:1, :]
                tail[pl.ds(pl.multiple_of(n * BLOCK, BLOCK), BLOCK), :] = jnp.exp(end - w + later).astype(BF16)
                prefix[0:1, :] = later + end
                return 0

            lax.fori_loop(0, TOK // BLOCK, back, 0)
            dec_send[0] = jnp.broadcast_to(jnp.exp(prefix[0:1, :]), (8, 2 * KEY))

        def project(self, g, p, k):
            w, acc = bufs[g][p], (acc_a, acc_b)[p]
            u = ((z if p == 0 else y) + DELTA[k]) % 4
            if p == 0:
                lhs = xs[:, pl.ds(pl.multiple_of(u * 1024, 1024), 1024)]
            else:
                lhs = jnp.concatenate(
                    [xs[:, pl.ds(pl.multiple_of((v * 4 + u) * KB, KB), KB)] for v in range(4)], axis=1
                )
            cols = lanes[g]
            part = mm(lhs, w[pl.ds(pl.multiple_of(first_row[g][p] + u * 1024, 1024), 1024), cols])
            if k == 0:
                acc[:, cols] = part
            else:
                acc[:, cols] += part

        def key_state(self):
            def step(i, _):
                r = pl.ds(pl.multiple_of(i * 64, 64), 64)
                krows[r, :] = acc_a[r, 0:256].astype(BF16)
                vrows[r, 0:128] = acc_a[r, 256:384].astype(BF16)
                vrows[r, 128:512] = acc_b[r, 0:384].astype(BF16)
                return 0

            lax.fori_loop(0, TOK // 64, step, 0)
            k_tail = (krows[...].astype(F32) * tail[...].astype(F32)).astype(BF16)
            for h in range(2):
                kc, vc = head(h)
                s = tn(vrows[:, vc], k_tail[:, kc])
                st_send[0, vc, :] = s.astype(BF16)
            state[...] = jnp.zeros_like(state)
            prefix[0:1, :] = jnp.zeros((1, 2 * KEY), F32)

        def attend(self, lo, hi):
            def step(n, _):
                r = pl.ds(pl.multiple_of(n * BLOCK, BLOCK), BLOCK)
                row = lax.broadcasted_iota(jnp.int32, (BLOCK, BLOCK), 0)
                col = lax.broadcasted_iota(jnp.int32, (BLOCK, BLOCK), 1)
                causal = row >= col
                w = within[r, :]
                end = w[BLOCK - 1 : BLOCK, :]
                mid = end * 0.5
                q_now = jnp.concatenate([acc_a[r, 384:512], acc_b[r, 384:512]], axis=1).astype(BF16)
                q_s = q_now.astype(F32) * (KEY**-0.5) * jnp.exp(w - mid)
                k_s = krows[r, :].astype(F32) * jnp.exp(mid - w)
                e_mid = jnp.exp(mid)
                q_d = q_s * e_mid
                k_t = (k_s * e_mid).astype(BF16)
                e_end = jnp.exp(end)
                before = prefix[0:1, :]
                q_far[r, :] = (q_d * jnp.exp(before)).astype(BF16)
                prefix[0:1, :] = before + end
                q_d = q_d.astype(BF16)
                q_s = q_s.astype(BF16)
                k_s = k_s.astype(BF16)
                for h in range(2):
                    kc, vc = head(h)
                    v = vrows[r, vc]
                    scores = jnp.where(causal, nt(q_s[:, kc], k_s[:, kc]), 0.0).astype(BF16)
                    s = state[vc, :]
                    inside[r, vc] = mm(scores, v) + nt(q_d[:, kc], s.astype(BF16))
                    state[vc, :] = s * e_end[:, kc] + tn(v, k_t[:, kc])
                return 0

            lax.fori_loop(lo, hi, step, 0)

        def fold(self, total, decay, i, use):
            dec = jnp.where(use, dec_recv[i][0:1, :], 1.0)
            out_ = []
            for h in range(2):
                kc, vc = head(h)
                got = jnp.where(use, st_recv[i, vc, :].astype(F32), 0.0)
                out_.append(total[h] * dec[:, kc] + got)
            return out_, decay * dec

        def fold_y(self):
            own_decay = dec_send[0][0:1, :]
            total = [jnp.zeros((VAL, KEY), F32) for _ in range(2)]
            decay = jnp.ones((1, 2 * KEY), F32)
            for d in (3, 2, 1):
                total, decay = self.fold(total, decay, d - 1, d <= y)
            prefix[1:2, :] = decay
            for h in range(2):
                kc, vc = head(h)
                state[vc, :] = total[h]
                total[h] = total[h] * own_decay[:, kc] + st_send[0, vc, :].astype(F32)
            decay = decay * own_decay
            for d in (3, 2, 1):
                total, decay = self.fold(total, decay, d - 1, d > y)
            for h in range(2):
                kc, vc = head(h)
                st_send[1, vc, :] = total[h].astype(BF16)
            dec_send[1] = jnp.broadcast_to(decay, (8, 2 * KEY))

        def fold_z(self):
            total = [jnp.zeros((VAL, KEY), F32) for _ in range(2)]
            decay = jnp.ones((1, 2 * KEY), F32)
            for d in (3, 2, 1):
                total, decay = self.fold(total, decay, 3 + d - 1, d <= z)
            decay = prefix[1:2, :]
            for h in range(2):
                kc, vc = head(h)
                state[vc, :] = total[h] * decay[:, kc] + state[vc, :]
            hg = head_gain[...].astype(F32)

            def finish(g, _):
                r = pl.ds(pl.multiple_of(g * ROWS, 32), ROWS)
                to = self.place(g)
                for h in range(2):
                    kc, vc = head(h)
                    a = inside[r, vc] + nt(q_far[r, kc], state[vc, :].astype(BF16))
                    ms = jnp.mean(a * a, axis=-1, keepdims=True)
                    mix[to, vc] = (a * lax.rsqrt(ms + EPS) * hg[h : h + 1, :]).astype(BF16)
                return 0

            lax.fori_loop(0, 8, finish, 0)

        def place(self, g):
            mine = 1 - (g + core) % 2
            d = (g // 2 + 4 - xi) % 4
            return pl.ds(pl.multiple_of((mine * 4 + d) * ROWS, 32), ROWS)

        def gate(self, g):
            gated = gated_c if g == "c" else gated_d

            def rnd(v):
                return v.astype(BF16).astype(F32)

            def step(i, _):
                r = pl.ds(pl.multiple_of(i * 64, 64), 64)
                o = pl.ds(pl.multiple_of(i * 64 + 8, 8), 64)
                gated[o, 0:128] = rnd(rnd(acc_b[r, 256:384]) * rnd(acc_a[r, 128:256]))
                gated[o, 128:256] = rnd(rnd(acc_a[r, 0:128]) * rnd(acc_a[r, 256:384]))
                return 0

            lax.fori_loop(0, TOK // 64, step, 0)
            go(halo_copy(g))

        def rows(self, g, i):
            gated = gated_c if g == "c" else gated_d
            tp = taps[...].astype(F32)[:, slice(0, EARLY) if g == "c" else slice(EARLY, 512)]
            block = gated[pl.ds(pl.multiple_of(i * ROWS, 32), ROWS + 8), :]
            if isinstance(i, int):
                keep = jnp.where(sp == 0, 0.0, 1.0)
                rim = lax.broadcasted_iota(jnp.int32, (ROWS + 8, 1), 0) < 8
                block = jnp.where(rim, block * keep, block)
            one = pltpu.roll(block, 1, 0)[8:, :]
            two = pltpu.roll(block, 2, 0)[8:, :]
            s = tp[0:1, :] * two + tp[1:2, :] * one + tp[2:3, :] * block[8:, :]
            r = pl.ds(pl.multiple_of(i * ROWS, 32), ROWS)
            s = (s * acc_b[r, 0:256].astype(BF16).astype(F32)).astype(BF16)
            if g == "c":
                mix[self.place(i), 512:MIX] = s
            else:
                late_mix[r, :] = s

        def conv(self, g):
            def step(i, _):
                self.rows(g, i)
                return 0

            lax.fori_loop(1, 8, step, 0)

        def first_rows(self, g):
            halo_copy(g).wait_recv()
            self.rows(g, 0)

        def load_h(self):
            for c in started_q:
                c.wait_send()
            for c in h_loads():
                c.start()
            for to in (at_x(1), at_x(3), to_sib):
                pl.semaphore_signal(free_sem, inc=1, device_id=to, device_id_type=MESH)

        def start_h(self):
            for c in h_loads():
                c.wait()
            pl.semaphore_wait(free_sem, 3)

        def pair_products(self, i):
            for c in out_loads(i):
                c.wait()
            if i >= 2:
                sib_copy(i - 2).wait_send()
            sib_send[i % 2] = mm(mix[0 : 4 * ROWS, :], wo[i % 3]).astype(BF16)
            sib_copy(i).start()
            own[i % 4] = mm(mix[4 * ROWS : TOK, :], wo[i % 3])
            if i + 3 < CHUNKS:
                for c in out_loads(i + 3):
                    c.start()

        def pair(self, c, d, r0, rows):
            at = slice(d * ROWS + r0, d * ROWS + r0 + rows)
            return own[c % 4, at, :] + sib_recv[c, at, :].astype(F32)

        def far(self, c):
            sib_copy(c).wait_recv()
            for side in (0, 1):
                if c >= 4:
                    far_copy(c - 4, side).wait_send()
                far_send[c % 4, side] = self.pair(c, 2, side * 48, 48).astype(BF16)
                far_copy(c, side).start()

        def near(self, c):
            for side in (0, 1):
                d = 1 + 2 * side
                if c >= 4:
                    near_copy(c - 4, side).wait_send()
                far_copy(c, side).wait_recv()
                for half in (0, 1):
                    v = self.pair(c, d, 48 * half, 48)
                    if half == side:
                        v = v + far_recv[c, side].astype(F32)
                    near_send[c % 4, side, 48 * half : 48 * half + 48, :] = v.astype(BF16)
                near_copy(c, side).start()

        def gather(self, c):
            near_copy(c, 0).wait_recv()
            near_copy(c, 1).wait_recv()
            total = self.pair(c, 0, 0, ROWS) + near_recv[c, 0].astype(F32) + near_recv[c, 1].astype(F32)
            inside[c * ROWS : (c + 1) * ROWS, :] = total

        def exchange(self):
            for d in (1, 7, 2, 6, 3, 5, 4):
                go(late_copy(d, True))
            late_recv[t] = late_mix[pl.ds(own_rows, ROWS), :]

        def collect(self):
            for d in range(1, 8):
                late_copy(d, False).wait_recv()

        def last(self, i):
            k = slice(i * CW, (i + 1) * CW)
            lhs_f = jnp.concatenate([late_recv[g, :, 0:128] for g in range(8)], axis=1)
            lhs_h = jnp.concatenate([late_recv[g, :, 128:256] for g in range(8)], axis=1)
            w_h = jnp.concatenate([qab[g * 1024 + i * 128 : g * 1024 + (i + 1) * 128, :] for g in range(8)], axis=0)
            total = inside[i * ROWS : (i + 1) * ROWS, :] + mm(lhs_f, wf[:, k]) + mm(lhs_h, w_h)
            out[:, k] = total.astype(BF16)

        def close(self):
            for i in range(CHUNKS - 2, CHUNKS):
                sib_copy(i).wait_send()
            for i in range(CHUNKS - 4, CHUNKS):
                for side in (0, 1):
                    far_copy(i, side).wait_send()
                    near_copy(i, side).wait_send()
            for c in started:
                c.wait_send()

    device = Device()
    for kind, *what in ORDER:
        if kind == "run":
            getattr(device, what[0])(*what[1:])
        else:
            getattr(device, kind)(*what)
    device.close()


def layer(*args):
    any_ = pl.BlockSpec(memory_space=pl.ANY)
    vmem = pl.BlockSpec(memory_space=pltpu.VMEM)
    dma = pltpu.SemaphoreType.DMA

    def f32(*shape):
        return pltpu.VMEM(shape, F32)

    def bf16(*shape):
        return pltpu.VMEM(shape, BF16)

    return pl.pallas_call(
        layer_kernel,
        out_shape=pltpu.VMEM((ROWS, MODEL), BF16),
        in_specs=[any_, vmem] + [any_] * 6 + [vmem] * 6 + [any_] * 2,
        out_specs=vmem,
        scratch_shapes=[
            bf16(TOK, MODEL),
            bf16(2 * MODEL, 512),
            bf16(MODEL, 384),
            bf16(MODEL, 384),
            bf16(MODEL, 384),
            bf16(MODEL, 384),
            bf16(8 * 128, MODEL),
            bf16(3, MIX, CW),
            f32(TOK, 512),
            f32(TOK, 512),
            bf16(TOK, 2 * KEY),
            bf16(TOK, 2 * VAL),
            bf16(TOK, 64),
            f32(TOK, 2 * KEY),
            bf16(TOK, 2 * KEY),
            f32(8, TOK),
            f32(TOK, 2 * VAL),
            bf16(TOK, 2 * KEY),
            f32(2 * VAL, KEY),
            f32(8, 2 * KEY),
            bf16(2, 2 * VAL, KEY),
            f32(2, 8, 2 * KEY),
            bf16(6, 2 * VAL, KEY),
            f32(6, 8, 2 * KEY),
            f32(TOK + 8, EARLY),
            f32(TOK + 8, LATE),
            bf16(TOK, MIX),
            bf16(TOK, LATE),
            bf16(8, ROWS, LATE),
            f32(4, 4 * ROWS, CW),
            bf16(2, 4 * ROWS, CW),
            bf16(CHUNKS, 4 * ROWS, CW),
            bf16(4, 2, 48, CW),
            bf16(CHUNKS, 2, 48, CW),
            bf16(4, 2, ROWS, CW),
            bf16(CHUNKS, 2, ROWS, CW),
            dma((23,)),
            dma((2 * CHUNKS,)),
            dma((8, 20)),
            dma((8, 20)),
            dma((30,)),
            dma((30,)),
            dma((16,)),
            dma((16,)),
            dma((2,)),
            dma((2,)),
            dma((7,)),
            dma((7,)),
            dma((CHUNKS,)),
            dma((CHUNKS,)),
            dma((CHUNKS, 2)),
            dma((CHUNKS, 2)),
            dma((CHUNKS, 2)),
            dma((CHUNKS, 2)),
            pltpu.SemaphoreType.REGULAR,
        ],
        compiler_params=pltpu.CompilerParams(
            collective_id=0, has_side_effects=True, vmem_limit_bytes=66_100_000
        ),
        name="layer",
    )(*args)


def body(
    hidden_activations,
    entry_rescale_vector,
    probe_matrix,
    lookup_address_matrix,
    payload_matrix,
    postfilter_switch_matrix,
    prefilter_switch_matrix,
    filter_source_matrix,
    forget_left_factor,
    forget_right_factor,
    forget_offset_per_feature,
    forget_spike_additions,
    subspace_rescale_vector,
    depthwise_filter_taps,
    mixer_result_matrix,
    filter_result_matrix,
):
    return layer(
        hidden_activations,
        entry_rescale_vector.reshape(32, 128),
        probe_matrix,
        lookup_address_matrix,
        payload_matrix,
        postfilter_switch_matrix,
        prefilter_switch_matrix,
        filter_source_matrix,
        forget_left_factor.T,
        forget_right_factor,
        forget_offset_per_feature[None, :],
        forget_spike_additions,
        subspace_rescale_vector,
        depthwise_filter_taps,
        mixer_result_matrix,
        filter_result_matrix,
    )


def solution(mesh):
    split = Mesh(mesh.devices.reshape(4, 4, mesh.shape["tp"]), ("sp_0", "sp_1", "tp"))
    in_specs = (
        P(SP_TP, None),
        P(),
        P(SP, "tp"),
        P(SP, "tp"),
        P(SP, "tp"),
        P(SP, "tp"),
        P(SP, "tp"),
        P(SP, "tp"),
        P(),
        P(None, "tp"),
        P("tp"),
        P("tp", SP),
        P("tp", None),
        P(None, "tp"),
        P("tp", None),
        P("tp", None),
    )
    out_specs = P(SP_TP, None)
    return jax.shard_map(body, mesh=split, in_specs=in_specs, out_specs=out_specs, check_vma=False)
```
